128 devices in a mesh: grp: 4 (over y, x), ep: 32 (over z, core).
Axes of the slice: x: 2, y: 2, z: 16, core: 2. Of those that a mesh axis runs over, the one named last changes fastest.
The devices are a block of a 8x8x16 slice.
Arguments:
- hidden: bfloat16 [384, 2048], P(('grp', 'ep')), parts along dimension 0, may hold values from -6 to 6
- conv_window: bfloat16 [384, 3, 6144], P(('grp', 'ep')), parts along dimension 0, may hold values from -6 to 6
- ssm_state: float32 [384, 64, 64, 128], P(('grp', 'ep')), parts along dimension 0, may hold values from -1.75 to 1.75
- gate_proj: bfloat16 [2048, 4096], P(None, 'ep'), may hold values from -0.125 to 0.125
- input_proj: bfloat16 [2048, 4096], P(None, 'ep'), may hold values from -0.125 to 0.125
- write_proj: bfloat16 [2048, 1024], P(None, 'ep'), may hold values from -0.125 to 0.125
- read_proj: bfloat16 [2048, 1024], P(None, 'ep'), may hold values from -0.125 to 0.125
- step_proj: bfloat16 [2048, 64], replicated, may hold values from -0.125 to 0.125
- step_bias: float32 [64], replicated, may hold values from -2 to 1
- decay_log: float32 [64], replicated, may hold values from -2.3 to 1.4
- decay_shift: float32 [384, 64], P(('grp', 'ep')), parts along dimension 0, may hold values from -0.7 to 0
- skip_scale: float32 [64], replicated, may hold values from -4 to 4
- conv_taps: bfloat16 [4, 6144], replicated, may hold values from -3 to 3
- conv_bias: float32 [6144], replicated, may hold values from -3 to 3
- mix_gain: float32 [2048], replicated, may hold values from 0.1 to 1.9
- group_gain: float32 [4096], replicated, may hold values from 0.1 to 1.9
- out_proj: bfloat16 [4096, 2048], P(None, 'ep'), may hold values from -0.09375 to 0.09375
- ffn_gain: float32 [2048], replicated, may hold values from 0.1 to 1.9
- router: bfloat16 [2048, 32], replicated, may hold values from -0.125 to 0.125
- expert_ids: int32 [384, 6], P(('grp', 'ep')), parts along dimension 0, may hold values from 0 to 31, all different within a row; in each aligned block of 3 rows (0 to 2, 3 to 5, ...) at most 2 rows name the same one
- expert_gate: bfloat16 [32, 2048, 512], P('ep'), may hold values from -0.125 to 0.125
- expert_up: bfloat16 [32, 2048, 512], P('ep'), may hold values from -0.125 to 0.125
- expert_down: bfloat16 [32, 512, 2048], P('ep'), may hold values from -0.25 to 0.25
- shared_gate: bfloat16 [2048, 512], P('ep'), may hold values from -0.125 to 0.125
- shared_up: bfloat16 [2048, 512], P('ep'), may hold values from -0.125 to 0.125
- shared_down: bfloat16 [512, 2048], replicated, may hold values from -0.25 to 0.25
Outputs:
- layer_out: bfloat16 [384, 2048], P(('grp', 'ep')), parts along dimension 0
- next_state: float32 [384, 64, 64, 128], P(('grp', 'ep')), parts along dimension 0
- next_window: bfloat16 [384, 3, 6144], P(('grp', 'ep')), parts along dimension 0
The draws below stay inside these ranges and needn't reach their ends.
There are 4 independent parts, one for each index of `grp`. The reference program is written for one: setup_inputs(seed, part) draws one part's arguments, and reference() takes and returns one part's arrays. A program takes and returns all parts, laid end to end along the dimension named above; an argument that names none is the same for every part. Nothing has to cross between parts.
Inputs may be any that keep to these rules, and one draw needn't show every extreme that they name: `expert_ids`: each row names 6 different experts; in the rows of one device no expert is named by more than 2 rows, and in every draw some device's rows name some expert exactly 2 times.
All inputs are finite; a program needn't handle non-finite values.
Results may differ from the reference program's by a relative error of at most 0.019.
Values may be sent and summed in bfloat16 or wider, within the bound.
No kernel may reach another device: no remote copies, remote signals or barrier semaphores. Data moves between devices by JAX's collectives and lax.ppermute only.
A program may use at most 128 MiB of HBM per device.

```python
import math
import jax
import jax.numpy as jnp
import numpy as np
from jax import lax

D = 2048
INNER = 4096
HEAD_DIM = 64
GROUPS = 8
STATE = 128
CONV = 4
EFF = 512
SFF = 512
TOP_K = 6
SEQ_DEV = 3
CAP = 2
HEADS = 64
CONV_DIM = 6144
EXPERTS = 32
SEQS = 96


def block_levels(own_key, extent, shards, low, largest):
    loudness, own = 1.0, jax.random.fold_in(own_key, 6)
    for dim, shards_of in shards:
        draws = jnp.exp(jax.random.uniform(jax.random.fold_in(own, dim), (shards_of,), jnp.float32, low / len(shards), largest / len(shards)))
        loudness = loudness * jnp.repeat(draws, extent[dim] // shards_of).reshape([-1 if axis == dim else 1 for axis in range(len(extent))])
    return loudness


def routed_block(rng, own, number, rows, amount, top, limit, slope):
    order = jax.random.permutation(rng, amount)
    packed, ordinary = shares(amount, rows * top, limit, slope, True), shares(amount, rows * top, limit, slope, False)
    places = jnp.arange(amount)

    def named(lengths, offset_by):
        used = int((lengths > 0).sum())
        fixed = max(1, used // 4)
        passed = fixed + (places - fixed + offset_by * (used - fixed)) % max(1, amount - fixed)
        return jnp.zeros((amount,), jnp.int32).at[order[jnp.where(places < fixed, places, passed)]].set(jnp.asarray(lengths, jnp.int32))

    lengths = jnp.where(number % 4 == 0, named(packed, number // 4), named(ordinary, number - number // 4 - 1))
    mixed = jax.random.permutation(jax.random.fold_in(own, 3), amount)
    source_of, sink = mixed[0:amount // 2 * 2:2], mixed[1:amount // 2 * 2:2]
    slack = jnp.minimum(lengths[source_of] - 1, limit - lengths[sink]) // 2
    slack = jnp.where((source_of == order[0]) | (sink == order[0]) | (lengths[sink] == 0), 0, jnp.maximum(slack, 0))
    passed = jax.random.randint(jax.random.fold_in(own, 4), (amount // 2,), 0, 1 << 20) % (slack + 1)
    lengths = lengths.at[source_of].add(-passed).at[sink].add(passed)
    labels = jnp.searchsorted(jnp.cumsum(lengths), jnp.arange(rows * top), side="right").astype(jnp.int32)
    listing = labels.reshape(top, rows).T
    listing = listing[jax.random.permutation(jax.random.fold_in(own, 1), rows)]
    offset_by = jax.random.randint(jax.random.fold_in(own, 2), (rows, 1), 0, top)
    return jnp.take_along_axis(listing, (jnp.arange(top)[None, :] + offset_by) % top, axis=1)


def shares(count, total, most, lean, full):
    portions = [(1 << 20) // math.isqrt(grade ** lean) + 1 for grade in range(1, count + 1)]
    largest = most if full else min(most, max(-(-total // count), total * portions[0] // sum(portions)))
    least = 1 if total - largest >= count - 1 else 0
    given, rest = [largest] + [least] * (count - 1), total - largest - least * (count - 1)
    while rest > 0:
        free = [i for i in range(1, count) if given[i] < largest] or [i for i in range(1, count) if given[i] < most]
        pool, budget = sum([portions[i] for i in free]), rest
        for i in free:
            addition = min(most - given[i], max(1, budget * portions[i] // pool), rest)
            given[i] = given[i] + addition
            rest = rest - addition
    return np.array(given)


def gaussian(key, extent, deviation, most, pieces=(), held_as=jnp.bfloat16):
    values = deviation * jax.random.normal(key, extent, jnp.float32)
    if pieces:
        values = values * block_levels(key, extent, pieces, -0.22, 0.18)
    return jnp.clip(values, -most, most).astype(held_as)


def setup_inputs(seed: int = 0, part: int = 0) -> dict:
    seeds = jax.random.split(jax.random.key(seed), 27)
    part_keys = jax.random.split(jax.random.fold_in(seeds[26], part), 27)
    hidden = gaussian(part_keys[0], (SEQS, D), 1.0, 6.0, ((0, 32),))
    conv_window = gaussian(part_keys[1], (SEQS, CONV - 1, CONV_DIM), 1.0, 6.0, ((0, 32),))
    ssm_state = gaussian(part_keys[2], (SEQS, HEADS, HEAD_DIM, STATE), 0.3, 1.75, ((0, 32),), jnp.float32)
    gate_proj = gaussian(seeds[3], (D, INNER), D ** -0.5, 0.125, ((1, 32),))
    input_proj = gaussian(seeds[4], (D, INNER), D ** -0.5, 0.125, ((1, 32),))
    write_proj = gaussian(seeds[5], (D, GROUPS * STATE), D ** -0.5, 0.125, ((1, 32),))
    read_proj = gaussian(seeds[6], (D, GROUPS * STATE), D ** -0.5, 0.125, ((1, 32),))
    step_proj = gaussian(seeds[7], (D, HEADS), D ** -0.5, 0.125)
    step_bias = jnp.clip(jax.random.uniform(seeds[8], (HEADS,), jnp.float32, -2.0, 1.0), -2.0, 1.0)
    decay_log = jnp.clip(jax.random.uniform(seeds[9], (HEADS,), jnp.float32, -2.3, 1.4), -2.3, 1.4)
    decay_shift = jnp.clip(-0.7 + 0.7 * jax.random.uniform(part_keys[10], (SEQS, HEADS), jnp.float32) ** block_levels(part_keys[10], (SEQS, HEADS), ((0, 32),), -0.2, 0.2), -0.7, 0.0)
    skip_scale = gaussian(seeds[11], (HEADS,), 1.0, 4.0, (), jnp.float32)
    conv_taps = gaussian(seeds[12], (CONV, CONV_DIM), CONV ** -0.5, 3.0)
    conv_bias = gaussian(seeds[13], (CONV_DIM,), 0.5, 3.0, (), jnp.float32)
    mix_gain = jnp.clip(1.0 + 0.18 * jax.random.normal(seeds[14], (D,), jnp.float32), 0.1, 1.9)
    group_gain = jnp.clip(1.0 + 0.18 * jax.random.normal(seeds[15], (INNER,), jnp.float32), 0.1, 1.9)
    out_proj = gaussian(seeds[16], (INNER, D), INNER ** -0.5, 0.09375, ((1, 32),))
    ffn_gain = jnp.clip(1.0 + 0.18 * jax.random.normal(seeds[17], (D,), jnp.float32), 0.1, 1.9)
    router = gaussian(seeds[18], (D, EXPERTS), D ** -0.5, 0.125)
    expert_ids_keys = jax.random.split(jax.random.fold_in(part_keys[19], 1), SEQS // SEQ_DEV)
    expert_ids_turns = jax.random.permutation(jax.random.fold_in(part_keys[19], 3), SEQS // SEQ_DEV)
    expert_ids = jax.vmap(lambda own, number: routed_block(jax.random.fold_in(part_keys[19], 2), own, number, SEQ_DEV, EXPERTS, TOP_K, CAP, 2))(expert_ids_keys, expert_ids_turns).reshape((SEQS, TOP_K))
    expert_gate = gaussian(seeds[20], (EXPERTS, D, EFF), D ** -0.5, 0.125, ((0, 32),))
    expert_up = gaussian(seeds[21], (EXPERTS, D, EFF), D ** -0.5, 0.125, ((0, 32),))
    expert_down = gaussian(seeds[22], (EXPERTS, EFF, D), EFF ** -0.5, 0.25, ((0, 32),))
    shared_gate = gaussian(seeds[23], (D, SFF), D ** -0.5, 0.125, ((0, 32),))
    shared_up = gaussian(seeds[24], (D, SFF), D ** -0.5, 0.125, ((0, 32),))
    shared_down = gaussian(seeds[25], (SFF, D), SFF ** -0.5, 0.25)
    return {"hidden": hidden, "conv_window": conv_window, "ssm_state": ssm_state, "gate_proj": gate_proj, "input_proj": input_proj, "write_proj": write_proj, "read_proj": read_proj, "step_proj": step_proj, "step_bias": step_bias, "decay_log": decay_log, "decay_shift": decay_shift, "skip_scale": skip_scale, "conv_taps": conv_taps, "conv_bias": conv_bias, "mix_gain": mix_gain, "group_gain": group_gain, "out_proj": out_proj, "ffn_gain": ffn_gain, "router": router, "expert_ids": expert_ids, "expert_gate": expert_gate, "expert_up": expert_up, "expert_down": expert_down, "shared_gate": shared_gate, "shared_up": shared_up, "shared_down": shared_down}


epsilon = 1e-06
routed_scale = 2.5

def row_scale(values):
    return lax.rsqrt(lax.optimization_barrier(jnp.mean(values * values, axis=-1, keepdims=True)) + epsilon)

def matmul(left, right):
    return jnp.dot(left, right, preferred_element_type=jnp.float32)

def reference(hidden, conv_window, ssm_state, gate_proj, input_proj, write_proj, read_proj, step_proj, step_bias, decay_log, decay_shift, skip_scale, conv_taps, conv_bias, mix_gain, group_gain, out_proj, ffn_gain, router, expert_ids, expert_gate, expert_up, expert_down, shared_gate, shared_up, shared_down):
    batch_rows = hidden.shape[0]
    head_count = step_bias.shape[0]
    per_group = head_count // GROUPS
    inner_width = gate_proj.shape[1]
    state_span = GROUPS * STATE
    hidden_wide = hidden.astype(jnp.float32)
    normed = (hidden_wide * row_scale(hidden_wide) * mix_gain).astype(jnp.bfloat16)
    gate_rows = matmul(normed, gate_proj).astype(jnp.bfloat16)
    input_rows = matmul(normed, input_proj).astype(jnp.bfloat16)
    write_rows = matmul(normed, write_proj).astype(jnp.bfloat16)
    read_rows = matmul(normed, read_proj).astype(jnp.bfloat16)
    step_raw = matmul(normed, step_proj)
    fresh_row = jnp.concatenate([input_rows, write_rows, read_rows], axis=1)
    window = jnp.concatenate([conv_window, fresh_row[:, None, :]], axis=1)
    convolved = jax.nn.silu(lax.optimization_barrier(jnp.sum(window.astype(jnp.float32) * conv_taps.astype(jnp.float32)[None], axis=1)) + conv_bias)
    head_input = convolved[:, :inner_width].reshape(batch_rows, GROUPS, per_group, HEAD_DIM)
    write_vec = convolved[:, inner_width:inner_width + state_span].reshape(batch_rows, GROUPS, STATE)
    read_vec = convolved[:, inner_width + state_span:].reshape(batch_rows, GROUPS, STATE)
    step_size = jax.nn.softplus(step_raw + step_bias)
    decay_rate = jnp.exp(decay_shift - step_size * jnp.exp(decay_log)).reshape(batch_rows, GROUPS, per_group)
    step_group = step_size.reshape(batch_rows, GROUPS, per_group)
    carried = ssm_state.reshape(batch_rows, GROUPS, per_group, HEAD_DIM, STATE)
    next_state = decay_rate[..., None, None] * carried + (step_group[..., None] * head_input)[..., None] * write_vec[:, :, None, None, :]
    mixed_out = jnp.einsum('sgepn,sgn->sgep', next_state, read_vec, precision=lax.Precision.HIGHEST)
    mixed_out = mixed_out + skip_scale.reshape(GROUPS, per_group)[None, :, :, None] * head_input
    mixed_out = mixed_out.reshape(batch_rows, inner_width).astype(jnp.bfloat16)
    gated_out = mixed_out.astype(jnp.float32) * jax.nn.silu(gate_rows.astype(jnp.float32))
    blocks = gated_out.reshape(batch_rows, GROUPS, -1)
    gated_out = ((blocks * row_scale(blocks)).reshape(batch_rows, inner_width) * group_gain).astype(jnp.bfloat16)
    resid = (hidden_wide + matmul(gated_out, out_proj)).astype(jnp.bfloat16)
    resid_wide = resid.astype(jnp.float32)
    norm_scale = row_scale(resid_wide)
    routed_in = (resid_wide * norm_scale * ffn_gain).astype(jnp.bfloat16)
    shared_in = (resid_wide * ffn_gain).astype(jnp.bfloat16)
    scores = jax.nn.sigmoid(matmul(routed_in, router))
    picked = jnp.take_along_axis(scores, expert_ids, axis=1)
    weights = routed_scale * picked / lax.optimization_barrier(jnp.sum(picked, axis=1, keepdims=True))

    def add_expert(running, inputs):
        weight_gate, weight_up, weight_down, index = inputs
        expert_hidden = (jax.nn.silu(matmul(routed_in, weight_gate)) * matmul(routed_in, weight_up)).astype(jnp.bfloat16)
        result = matmul(expert_hidden, weight_down).astype(jnp.bfloat16)
        coefficient = lax.optimization_barrier(jnp.sum(jnp.where(expert_ids == index, weights, 0.0), axis=1))
        return (running + coefficient[:, None] * result.astype(jnp.float32), None)
    routed, _ = lax.scan(add_expert, jnp.zeros((batch_rows, hidden.shape[1]), jnp.float32), (expert_gate, expert_up, expert_down, jnp.arange(expert_gate.shape[0], dtype=jnp.int32)))
    shared_hidden = (jax.nn.silu(norm_scale * matmul(shared_in, shared_gate)) * (norm_scale * matmul(shared_in, shared_up))).astype(jnp.bfloat16)
    layer_out = (resid_wide + routed + matmul(shared_hidden, shared_down)).astype(jnp.bfloat16)
    return (layer_out, next_state.reshape(ssm_state.shape), window[:, 1:])
```

```python
import jax
import jax.numpy as jnp
from jax import lax
from jax.sharding import Mesh
from jax.sharding import PartitionSpec as P

HEAD_DIM = 64
GROUPS = 8
STATE = 128
CAP = 2
EP = ("zh", "zl", "core")
NEAR = ("zl", "core")
GRP_EP = ("grp",) + EP

epsilon = 1e-06
routed_scale = 2.5


def row_scale(values):
    return lax.rsqrt(jnp.mean(values * values, axis=-1, keepdims=True) + epsilon)


def matmul(left, right):
    return jnp.dot(left, right, preferred_element_type=jnp.float32)


def contract(left, right, left_dim, right_dim):
    return lax.dot_general(
        left, right, (((left_dim,), (right_dim,)), ((), ())), preferred_element_type=jnp.float32
    )


def split_pair(values):
    high = values.astype(jnp.bfloat16)
    low = (values - high.astype(jnp.float32)).astype(jnp.bfloat16)
    return high, low


def shards(
    hidden,
    conv_window,
    ssm_state,
    gate_proj,
    input_proj,
    write_proj,
    read_proj,
    step_proj,
    step_bias,
    decay_log,
    decay_shift,
    skip_scale,
    conv_taps,
    conv_bias,
    mix_gain,
    group_gain,
    out_proj,
    ffn_gain,
    router,
    expert_ids,
    expert_gate,
    expert_up,
    expert_down,
    shared_gate,
    shared_up,
    shared_down,
):
    rows = hidden.shape[0]
    width = hidden.shape[1]
    index = lax.axis_index(EP)
    count = lax.axis_size(EP)
    near = lax.axis_size(NEAR)
    experts = router.shape[1]
    units = shared_gate.shape[1]
    features = shared_gate.shape[0]
    near_units = units // near

    near_weights = jnp.concatenate(
        [
            jnp.moveaxis(shared_gate.reshape(features, near, near_units), 1, 0),
            jnp.moveaxis(shared_up.reshape(features, near, near_units), 1, 0),
        ],
        axis=2,
    )
    near_weights = lax.all_to_all(near_weights, NEAR, 0, 0, tiled=True)
    near_weights = near_weights.reshape(near * features, 2 * near_units)

    gathered = lax.all_gather(hidden, EP)
    gathered_wide = jnp.moveaxis(gathered, 0, 1).reshape(rows * count, width).astype(jnp.float32)
    normed = (gathered_wide * row_scale(gathered_wide) * mix_gain).astype(jnp.bfloat16)
    member = jnp.any(
        expert_ids[:, :, None] == jnp.arange(experts, dtype=jnp.int32)[None, None, :], axis=1
    )
    parts = jnp.concatenate(
        [
            matmul(normed, gate_proj).astype(jnp.bfloat16),
            matmul(normed, input_proj).astype(jnp.bfloat16),
            matmul(normed, write_proj).astype(jnp.bfloat16),
            matmul(normed, read_proj).astype(jnp.bfloat16),
        ],
        axis=1,
    )
    parts = jnp.moveaxis(parts.reshape(rows, count, -1), 1, 0)
    named = member.astype(jnp.bfloat16).T.reshape(count, rows, 1)
    pieces = lax.all_to_all(jnp.concatenate([parts, named], axis=2), EP, 0, 0, tiled=True)

    hidden_wide = hidden.astype(jnp.float32)
    normed_local = (hidden_wide * row_scale(hidden_wide) * mix_gain).astype(jnp.bfloat16)
    step_raw = matmul(normed_local, step_proj)

    widths = [gate_proj.shape[1], input_proj.shape[1], write_proj.shape[1], read_proj.shape[1]]
    fields, start = [], 0
    for size in widths:
        fields.append(
            jnp.moveaxis(pieces[:, :, start : start + size], 0, 1).reshape(rows, count * size)
        )
        start += size
    gate_rows, input_rows, write_rows, read_rows = fields
    chosen = pieces[:, :, start].T.reshape(1, rows * count)

    inner_width = gate_rows.shape[1]
    state_span = GROUPS * STATE
    head_count = step_bias.shape[0]
    per_group = head_count // GROUPS
    fresh_row = jnp.concatenate([input_rows, write_rows, read_rows], axis=1)
    window = jnp.concatenate([conv_window, fresh_row[:, None, :]], axis=1)
    convolved = jax.nn.silu(
        jnp.sum(window.astype(jnp.float32) * conv_taps.astype(jnp.float32)[None], axis=1)
        + conv_bias
    )
    head_input = convolved[:, :inner_width].reshape(rows, GROUPS, per_group, HEAD_DIM)
    write_vec = convolved[:, inner_width : inner_width + state_span].reshape(rows, GROUPS, STATE)
    read_vec = convolved[:, inner_width + state_span :].reshape(rows, GROUPS, STATE)
    step_size = jax.nn.softplus(step_raw + step_bias)
    decay_rate = jnp.exp(decay_shift - step_size * jnp.exp(decay_log)).reshape(
        rows, GROUPS, per_group
    )
    step_group = step_size.reshape(rows, GROUPS, per_group)
    carried = ssm_state.reshape(rows, GROUPS, per_group, HEAD_DIM, STATE)
    next_state = (
        decay_rate[..., None, None] * carried
        + (step_group[..., None] * head_input)[..., None] * write_vec[:, :, None, None, :]
    )
    mixed_out = jnp.einsum("sgepn,sgn->sgep", next_state, read_vec)
    mixed_out = mixed_out + skip_scale.reshape(GROUPS, per_group)[None, :, :, None] * head_input
    mixed_out = mixed_out.reshape(rows, inner_width).astype(jnp.bfloat16)
    gated_out = mixed_out.astype(jnp.float32) * jax.nn.silu(gate_rows.astype(jnp.float32))
    blocks = gated_out.reshape(rows, GROUPS, -1)
    gated_out = ((blocks * row_scale(blocks)).reshape(rows, inner_width) * group_gain).astype(
        jnp.bfloat16
    )

    col_width = out_proj.shape[1]
    gated_all = jnp.moveaxis(lax.all_gather(gated_out, EP), 0, 1).reshape(rows * count, inner_width)
    resid_cols = lax.dynamic_slice_in_dim(gathered_wide, index * col_width, col_width, 1).T
    resid_part = (resid_cols + contract(out_proj, gated_all, 0, 1)).astype(jnp.bfloat16)
    resid_all = lax.all_gather(resid_part, EP).reshape(width, rows * count)

    resid_wide = resid_all.astype(jnp.float32)
    norm_all = lax.rsqrt(jnp.mean(resid_wide * resid_wide, axis=0, keepdims=True) + epsilon)
    routed_in = (resid_wide * norm_all * ffn_gain[:, None]).astype(jnp.bfloat16)
    shared_in = (resid_wide * ffn_gain[:, None]).astype(jnp.bfloat16)

    order = jnp.arange(rows * count, dtype=jnp.int32)[None]
    chosen_rows = chosen.reshape(rows, count)
    earlier = (jnp.cumsum(chosen_rows, axis=0) - chosen_rows).reshape(1, rows * count)
    slot = jnp.arange(CAP * count, dtype=jnp.int32)[:, None]
    pick = (
        (slot % count == order % count)
        & (chosen > 0.5)
        & (earlier.astype(jnp.int32) == slot // count)
    ).astype(jnp.bfloat16)
    expert_hidden = (
        jax.nn.silu(contract(routed_in, expert_gate[0], 0, 0))
        * contract(routed_in, expert_up[0], 0, 0)
    ).astype(jnp.bfloat16)
    expert_rows = matmul(pick, expert_hidden).astype(jnp.bfloat16)
    result = matmul(expert_rows, expert_down[0]).astype(jnp.bfloat16)

    block = near * features
    shared_block = lax.dynamic_slice_in_dim(shared_in, (index // near) * block, block, 0)
    shared_part = contract(shared_block, near_weights, 0, 0).astype(jnp.bfloat16)
    shared_part = shared_part.reshape(rows, count, 2, near_units)
    shared_part = shared_part.transpose(1, 2, 0, 3).reshape(count, CAP, rows * near_units)
    outbound = jnp.concatenate(
        [jnp.moveaxis(result.reshape(CAP, count, width), 1, 0), shared_part], axis=2
    )
    returned = lax.all_to_all(outbound, EP, 0, 0, tiled=True)

    own = (
        jnp.arange(rows * count, dtype=jnp.int32)[None]
        == jnp.arange(rows, dtype=jnp.int32)[:, None] * count + index
    ).astype(jnp.bfloat16)
    resid_own = contract(own, resid_all, 1, 1)
    norm_scale = row_scale(resid_own)
    routed_own = (resid_own * norm_scale * ffn_gain).astype(jnp.bfloat16)
    scores = jnp.where(member, jax.nn.sigmoid(matmul(routed_own, router)), 0.0)
    weights = routed_scale * scores / jnp.sum(scores, axis=1, keepdims=True)
    own_member = member.astype(jnp.int32)
    own_slot = jnp.cumsum(own_member, axis=0) - own_member
    by_slot = jnp.concatenate([jnp.where(own_slot == s, weights, 0.0) for s in range(CAP)], axis=1)
    back = jnp.moveaxis(returned[:, :, :width], 1, 0).reshape(CAP * count, width)
    high, low = split_pair(by_slot)
    routed = matmul(high, back) + matmul(low, back)
    pre = returned[:, :, width:].reshape(count // near, near, 2, rows, near_units)
    pre = jnp.sum(pre.astype(jnp.float32), axis=0).transpose(1, 2, 0, 3).reshape(2, rows, units)
    shared_hidden = (jax.nn.silu(norm_scale * pre[0]) * (norm_scale * pre[1])).astype(jnp.bfloat16)
    layer_out = (resid_own + routed + matmul(shared_hidden, shared_down)).astype(jnp.bfloat16)
    return (layer_out, next_state.reshape(ssm_state.shape), window[:, 1:])


def solution(mesh):
    torus = Mesh(mesh.devices.reshape(mesh.shape["grp"], -1, 2, 2), GRP_EP)
    return jax.shard_map(
        shards,
        mesh=torus,
        in_specs=(
            P(GRP_EP, None),
            P(GRP_EP, None, None),
            P(GRP_EP, None, None, None),
            P(None, EP),
            P(None, EP),
            P(None, EP),
            P(None, EP),
            P(),
            P(),
            P(),
            P(GRP_EP, None),
            P(),
            P(),
            P(),
            P(),
            P(),
            P(None, EP),
            P(),
            P(),
            P(GRP_EP, None),
            P(EP, None, None),
            P(EP, None, None),
            P(EP, None, None),
            P(EP, None),
            P(EP, None),
            P(),
        ),
        out_specs=(P(GRP_EP, None), P(GRP_EP, None, None, None), P(GRP_EP, None, None)),
        check_vma=False,
    )
```

```python
import jax
import jax.numpy as jnp
from jax import lax
from jax.sharding import Mesh
from jax.experimental import pallas as pl
from jax.experimental.pallas import tpu as pltpu
from jax.sharding import PartitionSpec as P

HEAD_DIM = 64
GROUPS = 8
STATE = 128
CAP = 2
EP = ("zh", "zl", "core")
NEAR = ("zl", "core")
GRP_EP = ("grp",) + EP
NEAR_FIRST = NEAR + ("zh",)
SLAB = 4
LANES = 128

epsilon = 1e-06
routed_scale = 2.5


def row_scale(values):
    return lax.rsqrt(jnp.mean(values * values, axis=-1, keepdims=True) + epsilon)


def matmul(left, right):
    return jnp.dot(left, right, preferred_element_type=jnp.float32)


def contract(left, right, left_dim, right_dim):
    return lax.dot_general(
        left, right, (((left_dim,), (right_dim,)), ((), ())), preferred_element_type=jnp.float32
    )


def split_pair(values):
    high = values.astype(jnp.bfloat16)
    low = (values - high.astype(jnp.float32)).astype(jnp.bfloat16)
    return high, low


def near_gather(shard):
    count = lax.axis_size("zh")
    across = lax.all_to_all(
        jnp.broadcast_to(shard[None], (count, *shard.shape)), "zh", 0, 0, tiled=True
    )
    return lax.all_gather(across, NEAR)


def expert_kernel(
    place,
    resid,
    gain,
    chosen,
    near_weights,
    gate_hbm,
    up_hbm,
    down_hbm,
    out,
    own,
    gate,
    up,
    down,
    wide,
    routed,
    shared,
    partial,
    gate_sem,
    up_sem,
    down_sem,
):
    near, far, features, lanes = resid.shape
    width = near * far * features
    units = down.shape[0]
    half = width // 2
    copies = []
    for part in range(2):
        span = pl.ds(part * half, half)
        copies.append(
            (
                pltpu.make_async_copy(gate_hbm.at[0, span], gate.at[span], gate_sem.at[part]),
                pltpu.make_async_copy(up_hbm.at[0, span], up.at[span], up_sem.at[part]),
            )
        )
    down_copy = pltpu.make_async_copy(down_hbm.at[0], down, down_sem)
    for pair in copies:
        for copy in pair:
            copy.start()
    down_copy.start()

    square = jnp.zeros((lanes, 1), jnp.float32)
    for z in range(far):
        for pair in range(near // 2):
            block = jnp.concatenate([resid[2 * pair, z], resid[2 * pair + 1, z]], axis=0)
            rows = block.astype(jnp.float32).T
            start = (z * near + 2 * pair) * features
            wide[:, start : start + 2 * features] = rows
            square += jnp.sum(rows * rows, axis=1, keepdims=True)
    scale = lax.rsqrt(square / width + epsilon)
    values = wide[...]
    routed[...] = (values * scale * gain[...]).astype(jnp.bfloat16)
    shared[...] = (values * gain[...]).astype(jnp.bfloat16)

    me = place[0]
    count = chosen.shape[0]
    slabs = chosen.shape[1]
    for row in range(own.shape[0]):
        own[row : row + 1, :] = wide[pl.ds(me * slabs + row, 1), :]
    block = near * features
    start = pl.multiple_of((me // near) * block, block)
    pre = jnp.dot(
        shared[:, pl.ds(start, block)], near_weights[...], preferred_element_type=jnp.float32
    )
    for s in range(CAP):
        partial[s] = pre[:, s * LANES : (s + 1) * LANES]
    for s in range(CAP):
        for row in range(slabs):
            out[s * count : (s + 1) * count, width + row * LANES : width + (row + 1) * LANES] = (
                partial[s, pl.ds(row, count, stride=slabs), :]
            ).astype(jnp.bfloat16)

    gate_pre = jnp.zeros((lanes, units), jnp.float32)
    up_pre = jnp.zeros((lanes, units), jnp.float32)
    for part in range(2):
        span = slice(part * half, (part + 1) * half)
        for copy in copies[part]:
            copy.wait()
        gate_pre += jnp.dot(routed[:, span], gate[span], preferred_element_type=jnp.float32)
        up_pre += jnp.dot(routed[:, span], up[span], preferred_element_type=jnp.float32)
    expert_hidden = (gate_pre / (1.0 + jnp.exp(-gate_pre)) * up_pre).astype(jnp.bfloat16)

    lane = lax.broadcasted_iota(jnp.int32, (count, lanes), 1)
    line = lax.broadcasted_iota(jnp.int32, (count, lanes), 0)
    flags = chosen[...]
    down_copy.wait()
    for s in range(CAP):
        pick = jnp.zeros((count, lanes), jnp.float32)
        earlier = jnp.zeros((count, 1), jnp.float32)
        for row in range(slabs):
            flag = flags[:, row : row + 1]
            taken = jnp.where(earlier == float(s), flag, 0.0)
            pick = jnp.where(lane == line * slabs + row, taken, pick)
            earlier = earlier + flag
        rows = jnp.dot(
            pick.astype(jnp.bfloat16), expert_hidden, preferred_element_type=jnp.float32
        ).astype(jnp.bfloat16)
        out[s * count : (s + 1) * count, :width] = jnp.dot(
            rows, down[...], preferred_element_type=jnp.float32
        ).astype(jnp.bfloat16)


def expert_rows(place, resid, gain, chosen, near_weights, gate, up, down):
    near, far, features, lanes = resid.shape
    width = near * far * features
    units = down.shape[1]
    count, slabs = chosen.shape
    vmem = pl.BlockSpec(memory_space=pltpu.VMEM)
    hbm = pl.BlockSpec(memory_space=pltpu.HBM)
    return pl.pallas_call(
        expert_kernel,
        name="expert_rows",
        out_shape=(
            jax.ShapeDtypeStruct((CAP * count, width + slabs * LANES), jnp.bfloat16),
            jax.ShapeDtypeStruct((slabs, width), jnp.float32),
        ),
        in_specs=[pl.BlockSpec(memory_space=pltpu.SMEM), vmem, vmem, vmem, vmem, hbm, hbm, hbm],
        out_specs=(vmem, vmem),
        scratch_shapes=[
            pltpu.VMEM((width, units), jnp.bfloat16),
            pltpu.VMEM((width, units), jnp.bfloat16),
            pltpu.VMEM((units, width), jnp.bfloat16),
            pltpu.VMEM((lanes, width), jnp.float32),
            pltpu.VMEM((lanes, width), jnp.bfloat16),
            pltpu.VMEM((lanes, width), jnp.bfloat16),
            pltpu.VMEM((CAP, lanes, near_weights.shape[1] // CAP), jnp.float32),
            pltpu.SemaphoreType.DMA((2,)),
            pltpu.SemaphoreType.DMA((2,)),
            pltpu.SemaphoreType.DMA,
        ],
    )(place, resid, gain, chosen, near_weights, gate, up, down)


def shards(
    hidden,
    conv_window,
    ssm_state,
    gate_proj,
    input_proj,
    write_proj,
    read_proj,
    step_proj,
    step_bias,
    decay_log,
    decay_shift,
    skip_scale,
    conv_taps,
    conv_bias,
    mix_gain,
    group_gain,
    out_proj,
    ffn_gain,
    router,
    expert_ids,
    expert_gate,
    expert_up,
    expert_down,
    shared_gate,
    shared_up,
    shared_down,
):
    rows = hidden.shape[0]
    width = hidden.shape[1]
    index = lax.axis_index(EP)
    count = lax.axis_size(EP)
    near = lax.axis_size(NEAR)
    experts = router.shape[1]
    units = shared_gate.shape[1]
    features = shared_gate.shape[0]
    near_units = units // near

    near_weights = jnp.concatenate(
        [
            jnp.moveaxis(shared_gate.reshape(features, near, near_units), 1, 0),
            jnp.moveaxis(shared_up.reshape(features, near, near_units), 1, 0),
        ],
        axis=2,
    )
    near_weights = lax.all_to_all(near_weights, NEAR, 0, 0, tiled=True)
    near_weights = near_weights.reshape(near * features, 2 * near_units)

    slab = jnp.pad(hidden, ((0, SLAB - rows), (0, 0)))
    gathered_wide = near_gather(slab).reshape(count * SLAB, width).astype(jnp.float32)
    normed = (gathered_wide * row_scale(gathered_wide) * mix_gain).astype(jnp.bfloat16)
    member = jnp.any(
        expert_ids[:, :, None] == jnp.arange(experts, dtype=jnp.int32)[None, None, :], axis=1
    )
    parts = jnp.concatenate(
        [
            matmul(normed, gate_proj).astype(jnp.bfloat16),
            matmul(normed, input_proj).astype(jnp.bfloat16),
            matmul(normed, write_proj).astype(jnp.bfloat16),
            matmul(normed, read_proj).astype(jnp.bfloat16),
        ],
        axis=1,
    )
    far = lax.axis_size("zh")
    named = jnp.pad(member.astype(jnp.bfloat16), ((0, SLAB - rows), (0, 0)))
    named = named.reshape(SLAB, far, near).transpose(2, 1, 0).reshape(count, SLAB, 1)
    pieces = lax.all_to_all(
        jnp.concatenate([parts.reshape(count, SLAB, -1), named], axis=2),
        NEAR_FIRST,
        0,
        0,
        tiled=True,
    )
    pieces = pieces.reshape(near, far, SLAB, -1).transpose(1, 0, 2, 3).reshape(count, SLAB, -1)
    pieces = pieces[:, :rows]

    hidden_wide = hidden.astype(jnp.float32)
    normed_local = (hidden_wide * row_scale(hidden_wide) * mix_gain).astype(jnp.bfloat16)
    step_raw = matmul(normed_local, step_proj)

    widths = [gate_proj.shape[1], input_proj.shape[1], write_proj.shape[1], read_proj.shape[1]]
    fields, start = [], 0
    for size in widths:
        fields.append(
            jnp.moveaxis(pieces[:, :, start : start + size], 0, 1).reshape(rows, count * size)
        )
        start += size
    gate_rows, input_rows, write_rows, read_rows = fields
    chosen = pieces[:, :, start].astype(jnp.float32)

    inner_width = gate_rows.shape[1]
    state_span = GROUPS * STATE
    head_count = step_bias.shape[0]
    per_group = head_count // GROUPS
    fresh_row = jnp.concatenate([input_rows, write_rows, read_rows], axis=1)
    window = jnp.concatenate([conv_window, fresh_row[:, None, :]], axis=1)
    convolved = jax.nn.silu(
        jnp.sum(window.astype(jnp.float32) * conv_taps.astype(jnp.float32)[None], axis=1)
        + conv_bias
    )
    head_input = convolved[:, :inner_width].reshape(rows, GROUPS, per_group, HEAD_DIM)
    write_vec = convolved[:, inner_width : inner_width + state_span].reshape(rows, GROUPS, STATE)
    read_vec = convolved[:, inner_width + state_span :].reshape(rows, GROUPS, STATE)
    step_size = jax.nn.softplus(step_raw + step_bias)
    decay_rate = jnp.exp(decay_shift - step_size * jnp.exp(decay_log)).reshape(
        rows, GROUPS, per_group
    )
    step_group = step_size.reshape(rows, GROUPS, per_group)
    carried = ssm_state.reshape(rows, GROUPS, per_group, HEAD_DIM, STATE)
    next_state = (
        decay_rate[..., None, None] * carried
        + (step_group[..., None] * head_input)[..., None] * write_vec[:, :, None, None, :]
    )
    mixed_out = jnp.einsum("sgepn,sgn->sgep", next_state, read_vec)
    mixed_out = mixed_out + skip_scale.reshape(GROUPS, per_group)[None, :, :, None] * head_input
    mixed_out = mixed_out.reshape(rows, inner_width).astype(jnp.bfloat16)
    gated_out = mixed_out.astype(jnp.float32) * jax.nn.silu(gate_rows.astype(jnp.float32))
    blocks = gated_out.reshape(rows, GROUPS, -1)
    gated_out = ((blocks * row_scale(blocks)).reshape(rows, inner_width) * group_gain).astype(
        jnp.bfloat16
    )

    col_width = out_proj.shape[1]
    gated_all = lax.all_gather(gated_out, EP).reshape(count * rows, inner_width)
    resid_cols = lax.dynamic_slice_in_dim(gathered_wide, index * col_width, col_width, 1)
    resid_cols = resid_cols.reshape(near, far, SLAB, col_width)[:, :, :rows].transpose(3, 1, 0, 2)
    resid_cols = resid_cols.reshape(col_width, count * rows)
    resid_part = (resid_cols + contract(out_proj, gated_all, 0, 1)).astype(jnp.bfloat16)
    resid_part = jnp.pad(resid_part, ((0, 0), (0, LANES - count * rows)))
    resid_all = near_gather(resid_part)

    outbound, resid_own = expert_rows(
        index.astype(jnp.int32).reshape(1),
        resid_all,
        ffn_gain.reshape(1, width),
        chosen,
        near_weights,
        expert_gate,
        expert_up,
        expert_down,
    )
    outbound = jnp.moveaxis(outbound.reshape(CAP, count, -1), 1, 0)
    returned = lax.all_to_all(outbound, EP, 0, 0, tiled=True)

    norm_scale = row_scale(resid_own)
    routed_own = (resid_own * norm_scale * ffn_gain).astype(jnp.bfloat16)
    scores = jnp.where(member, jax.nn.sigmoid(matmul(routed_own, router)), 0.0)
    weights = routed_scale * scores / jnp.sum(scores, axis=1, keepdims=True)
    own_member = member.astype(jnp.int32)
    own_slot = jnp.cumsum(own_member, axis=0) - own_member
    by_slot = jnp.concatenate([jnp.where(own_slot == s, weights, 0.0) for s in range(CAP)], axis=1)
    back = jnp.moveaxis(returned[:, :, :width], 1, 0).reshape(CAP * count, width)
    high, low = split_pair(by_slot)
    routed = matmul(high, back) + matmul(low, back)
    pre = returned[:, :, width:].reshape(count // near, near, 2, rows, near_units)
    pre = jnp.sum(pre.astype(jnp.float32), axis=0).transpose(1, 2, 0, 3).reshape(2, rows, units)
    shared_hidden = (jax.nn.silu(norm_scale * pre[0]) * (norm_scale * pre[1])).astype(jnp.bfloat16)
    layer_out = (resid_own + routed + matmul(shared_hidden, shared_down)).astype(jnp.bfloat16)
    return (layer_out, next_state.reshape(ssm_state.shape), window[:, 1:])


def solution(mesh):
    torus = Mesh(mesh.devices.reshape(mesh.shape["grp"], -1, 2, 2), GRP_EP)
    return jax.shard_map(
        shards,
        mesh=torus,
        in_specs=(
            P(GRP_EP, None),
            P(GRP_EP, None, None),
            P(GRP_EP, None, None, None),
            P(None, EP),
            P(None, EP),
            P(None, EP),
            P(None, EP),
            P(),
            P(),
            P(),
            P(GRP_EP, None),
            P(),
            P(),
            P(),
            P(),
            P(),
            P(None, EP),
            P(),
            P(),
            P(GRP_EP, None),
            P(EP, None, None),
            P(EP, None, None),
            P(EP, None, None),
            P(EP, None),
            P(EP, None),
            P(),
        ),
        out_specs=(P(GRP_EP, None), P(GRP_EP, None, None, None), P(GRP_EP, None, None)),
        check_vma=False,
    )
```

```python
import jax
import jax.numpy as jnp
from jax import lax
from jax.sharding import Mesh
from jax.experimental import pallas as pl
from jax.experimental.pallas import tpu as pltpu
from jax.sharding import PartitionSpec as P

HEAD_DIM = 64
GROUPS = 8
STATE = 128
CAP = 2
EP = ("zh", "zl", "core")
NEAR = ("zl", "core")
GRP_EP = ("grp",) + EP
LANES = 128

epsilon = 1e-06
routed_scale = 2.5


def row_scale(values):
    return lax.rsqrt(jnp.mean(values * values, axis=-1, keepdims=True) + epsilon)


def matmul(left, right):
    return jnp.dot(left, right, preferred_element_type=jnp.float32)


def contract(left, right, left_dim, right_dim):
    return lax.dot_general(
        left, right, (((left_dim,), (right_dim,)), ((), ())), preferred_element_type=jnp.float32
    )


def split_pair(values):
    high = values.astype(jnp.bfloat16)
    low = (values - high.astype(jnp.float32)).astype(jnp.bfloat16)
    return high, low


def near_gather(shard):
    count = lax.axis_size("zh")
    across = lax.all_to_all(
        jnp.broadcast_to(shard[None], (count, *shard.shape)), "zh", 0, 0, tiled=True
    )
    return lax.all_gather(across, NEAR)


def kept_in(space, arrays):
    return [pltpu.with_memory_space_constraint(array, space) for array in arrays]


def fast_call(kernel, name, outs, scratch, scalars, fetched, arrays, far=()):
    vmem = pl.BlockSpec(memory_space=pltpu.VMEM)
    smem = pl.BlockSpec(memory_space=pltpu.SMEM)
    hbm = pl.BlockSpec(memory_space=pltpu.HBM)
    specs = [smem] * len(scalars) + [vmem] * (len(fetched) + len(arrays)) + [hbm] * len(far)
    landing = [pltpu.VMEM(array.shape, array.dtype) for array in far]
    waits = [pltpu.SemaphoreType.DMA((len(far),))] if far else []
    return pl.pallas_call(
        kernel,
        name=name,
        out_shape=tuple(pltpu.VMEM(shape, dtype) for shape, dtype in outs),
        in_specs=specs,
        out_specs=(vmem,) * len(outs),
        scratch_shapes=[pltpu.VMEM(shape, dtype) for shape, dtype in scratch] + landing + waits,
        compiler_params=pltpu.CompilerParams(vmem_limit_bytes=24 * 1024 * 1024),
    )(*scalars, *kept_in(pltpu.HBM, fetched), *kept_in(pltpu.VMEM, arrays), *kept_in(pltpu.HBM, far))


def open_kernel(hidden, gate, up, out, staged):
    rows, width = hidden.shape
    chunks = width // LANES
    values = hidden[...].astype(jnp.float32)
    for k in range(chunks):
        staged[pl.ds(k, rows, stride=chunks), :] = values[:, k * LANES : (k + 1) * LANES]
    mine = staged[...].astype(jnp.bfloat16)
    gates = gate[...].astype(jnp.float32)
    ups = up[...].astype(jnp.float32)
    count = out.shape[0]
    half = gate.shape[1] // count
    for z in range(count):
        span = slice(z * half, (z + 1) * half)
        out[z, : rows * chunks, :] = mine
        out[z, rows * chunks :, :] = jnp.concatenate(
            [gates[:, span], ups[:, span]], axis=1
        ).astype(jnp.bfloat16)


def project_kernel(
    place,
    ids,
    gain,
    gathered,
    gate_hbm,
    input_hbm,
    write_hbm,
    read_hbm,
    message,
    columns,
    flat,
    wide,
    normed,
    staged,
    gate_weights,
    input_weights,
    write_weights,
    read_weights,
    sems,
):
    copies = [
        pltpu.make_async_copy(gate_hbm, gate_weights, sems.at[0]),
        pltpu.make_async_copy(input_hbm, input_weights, sems.at[1]),
        pltpu.make_async_copy(write_hbm, write_weights, sems.at[2]),
        pltpu.make_async_copy(read_hbm, read_weights, sems.at[3]),
    ]
    for copy in copies:
        copy.start()
    near, far, chunk, lanes = gathered.shape
    count = near * far
    rows = ids.shape[0]
    blocks = chunk // rows
    lines = message.shape[1]
    flat[...] = gathered[...].reshape(count * chunk, lanes).astype(jnp.float32)
    square = jnp.zeros((rows * count, 1), jnp.float32)
    for k in range(blocks):
        for row in range(rows):
            for n in range(near):
                wide[k, pl.ds(row * count + n, far, stride=near), :] = flat[
                    pl.ds(n * far * chunk + row * blocks + k, far, stride=chunk), :
                ]
        part = wide[k]
        square += jnp.sum(part * part, axis=1, keepdims=True)
    scale = lax.rsqrt(square / (blocks * lanes) + epsilon)
    for k in range(blocks):
        span = slice(k * lanes, (k + 1) * lanes)
        normed[:, span] = (wide[k] * scale * gain[:, span]).astype(jnp.bfloat16)
    values = normed[...]
    for copy in copies:
        copy.wait()
    gate_part = jnp.dot(values, gate_weights[...], preferred_element_type=jnp.float32)
    input_part = jnp.dot(values, input_weights[...], preferred_element_type=jnp.float32)
    write_part = contract(values, write_weights[...], 1, 1)
    read_part = contract(values, read_weights[...], 1, 1)

    def of_row(part, row):
        return part[row * count : (row + 1) * count]

    small = lanes - rows * write_part.shape[1]
    expert = lax.broadcasted_iota(jnp.int32, (count, small), 0)
    lane = lax.broadcasted_iota(jnp.int32, (count, small), 1)
    member = jnp.zeros((count, small), jnp.float32)
    for row in range(rows):
        for k in range(ids.shape[1]):
            member = jnp.where((lane == row) & (expert == ids[row, k]), 1.0, member)
    for row in range(rows):
        staged[pl.ds(row, count, stride=lines), :] = of_row(gate_part, row)
        staged[pl.ds(rows + row, count, stride=lines), :] = of_row(input_part, row)
    staged[pl.ds(2 * rows, count, stride=lines), :] = jnp.concatenate(
        [of_row(write_part, row) for row in range(rows)] + [member], axis=1
    )
    staged[pl.ds(2 * rows + 1, count, stride=lines), :] = jnp.concatenate(
        [of_row(read_part, row) for row in range(rows)] + [jnp.zeros_like(member)], axis=1
    )
    message[...] = staged[...].astype(jnp.bfloat16).reshape(count, lines, lanes)

    me = place[0]
    height = columns.shape[0]
    across = jnp.concatenate(
        [wide[me * height // lanes], jnp.zeros((lanes - rows * count, lanes), jnp.float32)], axis=0
    ).T
    columns[...] = jnp.where(me % 2 == 0, across[:height], across[height:])


def expert_kernel(
    place,
    gain,
    resid,
    chosen,
    part,
    gate_hbm,
    up_hbm,
    down_hbm,
    out,
    own,
    wide,
    routed,
    shared,
    staged,
    spread,
    gate,
    up,
    down,
    sems,
):
    near, far, features, lanes = resid.shape
    width = near * far * features
    count, slabs = chosen.shape
    lines = out.shape[1]
    copies = [
        pltpu.make_async_copy(gate_hbm, gate, sems.at[0]),
        pltpu.make_async_copy(up_hbm, up, sems.at[1]),
        pltpu.make_async_copy(down_hbm, down, sems.at[2]),
    ]
    for copy in copies:
        copy.start()
    square = jnp.zeros((lanes, 1), jnp.float32)
    for z in range(far):
        for pair in range(near // 2):
            block = jnp.concatenate([resid[2 * pair, z], resid[2 * pair + 1, z]], axis=0)
            rows = block.astype(jnp.float32).T
            start = (z * near + 2 * pair) * features
            wide[:, start : start + 2 * features] = rows
            square += jnp.sum(rows * rows, axis=1, keepdims=True)
    scale = lax.rsqrt(square / width + epsilon)
    values = wide[...]
    routed[...] = (values * scale * gain[...]).astype(jnp.bfloat16)
    shared[...] = (values * gain[...]).astype(jnp.bfloat16)

    me = place[0]
    for row in range(slabs):
        own[row : row + 1, :] = wide[pl.ds(row * count + me, 1), :]
    spread[...] = jnp.zeros_like(spread)
    for z in range(far):
        start = pl.multiple_of((z * near + lax.rem(me, near)) * features, features)
        spread[pl.ds(start, features), :] = part[z]
    partial = jnp.dot(shared[...], spread[...], preferred_element_type=jnp.float32)
    chunks = width // LANES
    for row in range(slabs):
        staged[pl.ds(CAP * chunks + row, count, stride=lines), :] = partial[
            row * count : (row + 1) * count
        ]

    copies[0].wait()
    gate_pre = jnp.dot(routed[...], gate[0], preferred_element_type=jnp.float32)
    copies[1].wait()
    up_pre = jnp.dot(routed[...], up[0], preferred_element_type=jnp.float32)
    expert_hidden = (gate_pre / (1.0 + jnp.exp(-gate_pre)) * up_pre).astype(jnp.bfloat16)

    lane = lax.broadcasted_iota(jnp.int32, (count, lanes), 1)
    line = lax.broadcasted_iota(jnp.int32, (count, lanes), 0)
    flags = chosen[...]
    picks = []
    for s in range(CAP):
        pick = jnp.zeros((count, lanes), jnp.float32)
        earlier = jnp.zeros((count, 1), jnp.float32)
        for row in range(slabs):
            flag = flags[:, row : row + 1]
            taken = jnp.where(earlier == float(s), flag, 0.0)
            pick = jnp.where(lane == row * count + line, taken, pick)
            earlier = earlier + flag
        picks.append(pick)
    pick = jnp.concatenate(picks, axis=0).astype(jnp.bfloat16)
    rows = jnp.dot(pick, expert_hidden, preferred_element_type=jnp.float32).astype(jnp.bfloat16)
    copies[2].wait()
    result = jnp.dot(rows, down[0], preferred_element_type=jnp.float32)
    for s in range(CAP):
        for k in range(chunks):
            staged[pl.ds(s * chunks + k, count, stride=lines), :] = result[
                s * count : (s + 1) * count, k * LANES : (k + 1) * LANES
            ]
    used = CAP * chunks + slabs
    for k in range(used, lines):
        staged[pl.ds(k, count, stride=lines), :] = jnp.zeros((count, LANES), jnp.float32)
    out[...] = staged[...].astype(jnp.bfloat16).reshape(count, lines, LANES)


def shards(
    hidden,
    conv_window,
    ssm_state,
    gate_proj,
    input_proj,
    write_proj,
    read_proj,
    step_proj,
    step_bias,
    decay_log,
    decay_shift,
    skip_scale,
    conv_taps,
    conv_bias,
    mix_gain,
    group_gain,
    out_proj,
    ffn_gain,
    router,
    expert_ids,
    expert_gate,
    expert_up,
    expert_down,
    shared_gate,
    shared_up,
    shared_down,
):
    rows = hidden.shape[0]
    width = hidden.shape[1]
    index = lax.axis_index(EP)
    count = lax.axis_size(EP)
    near = lax.axis_size(NEAR)
    experts = router.shape[1]
    units = shared_gate.shape[1]
    features = shared_gate.shape[0]

    far = lax.axis_size("zh")
    chunks = width // LANES
    place = index.astype(jnp.int32).reshape(1)
    (opening,) = fast_call(
        open_kernel,
        "open_rows",
        [((far, rows * chunks + features, LANES), jnp.bfloat16)],
        [((rows * chunks, LANES), jnp.float32)],
        [],
        [hidden, shared_gate, shared_up],
        [],
    )
    opened = lax.all_to_all(opening, "zh", 0, 0, tiled=True)
    gathered = lax.all_gather(opened[:, : rows * chunks], NEAR)
    shared_weights = opened[:, rows * chunks :]
    col_width = out_proj.shape[1]
    message, resid_cols = fast_call(
        project_kernel,
        "project_rows",
        [((count, 8, LANES), jnp.bfloat16), ((col_width, LANES), jnp.float32)],
        [
            ((count * rows * chunks, LANES), jnp.float32),
            ((chunks, count * rows, LANES), jnp.float32),
            ((count * rows, width), jnp.bfloat16),
            ((count * 8, LANES), jnp.float32),
        ],
        [place, expert_ids],
        [mix_gain.reshape(1, width)],
        [gathered],
        [gate_proj, input_proj, write_proj.T, read_proj.T],
    )
    pieces = lax.all_to_all(message, EP, 0, 0, tiled=True)

    later = (hidden, conv_window, conv_taps, decay_shift, step_bias, decay_log)
    later, _ = lax.optimization_barrier((later, message))
    hidden_later, conv_window, conv_taps, decay_shift, step_bias, decay_log = later
    hidden_wide = hidden_later.astype(jnp.float32)
    normed_local = (hidden_wide * row_scale(hidden_wide) * mix_gain).astype(jnp.bfloat16)
    step_raw = matmul(normed_local, step_proj)

    gate_rows = jnp.moveaxis(pieces[:, :rows], 0, 1).reshape(rows, -1)
    input_rows = jnp.moveaxis(pieces[:, rows : 2 * rows], 0, 1).reshape(rows, -1)
    tail_width = rows * write_proj.shape[1]
    write_rows, read_rows = (
        jnp.moveaxis(pieces[:, 2 * rows + k, :tail_width].reshape(count, rows, -1), 0, 1).reshape(
            rows, -1
        )
        for k in range(2)
    )
    chosen = pieces[:, 2 * rows, tail_width : tail_width + rows].astype(jnp.float32)

    inner_width = gate_rows.shape[1]
    state_span = GROUPS * STATE
    head_count = step_bias.shape[0]
    per_group = head_count // GROUPS
    fresh_row = jnp.concatenate([input_rows, write_rows, read_rows], axis=1)
    window = jnp.concatenate([conv_window, fresh_row[:, None, :]], axis=1)
    convolved = jax.nn.silu(
        jnp.sum(window.astype(jnp.float32) * conv_taps.astype(jnp.float32)[None], axis=1)
        + conv_bias
    )
    head_input = convolved[:, :inner_width].reshape(rows, GROUPS, per_group, HEAD_DIM)
    write_vec = convolved[:, inner_width : inner_width + state_span].reshape(rows, GROUPS, STATE)
    read_vec = convolved[:, inner_width + state_span :].reshape(rows, GROUPS, STATE)
    step_size = jax.nn.softplus(step_raw + step_bias)
    decay_rate = jnp.exp(decay_shift - step_size * jnp.exp(decay_log)).reshape(
        rows, GROUPS, per_group
    )
    step_group = step_size.reshape(rows, GROUPS, per_group)
    carried = ssm_state.reshape(rows, GROUPS, per_group, HEAD_DIM, STATE)
    next_state = (
        decay_rate[..., None, None] * carried
        + (step_group[..., None] * head_input)[..., None] * write_vec[:, :, None, None, :]
    )
    mixed_out = jnp.einsum("sgepn,sgn->sgep", next_state, read_vec)
    mixed_out = mixed_out + skip_scale.reshape(GROUPS, per_group)[None, :, :, None] * head_input
    mixed_out = mixed_out.reshape(rows, inner_width).astype(jnp.bfloat16)
    gated_out = mixed_out.astype(jnp.float32) * jax.nn.silu(gate_rows.astype(jnp.float32))
    blocks = gated_out.reshape(rows, GROUPS, -1)
    gated_out = ((blocks * row_scale(blocks)).reshape(rows, inner_width) * group_gain).astype(
        jnp.bfloat16
    )

    gated_all = jnp.moveaxis(lax.all_gather(gated_out, EP), 0, 1).reshape(rows * count, inner_width)
    resid_part = (resid_cols[:, : rows * count] + contract(out_proj, gated_all, 0, 1)).astype(
        jnp.bfloat16
    )
    resid_part = jnp.pad(resid_part, ((0, 0), (0, LANES - count * rows)))
    resid_all = near_gather(resid_part)
    used = CAP * chunks + rows
    outbound, resid_own = fast_call(
        expert_kernel,
        "expert_rows",
        [((count, -(-used // 8) * 8, LANES), jnp.bfloat16), ((rows, width), jnp.float32)],
        [
            ((LANES, width), jnp.float32),
            ((LANES, width), jnp.bfloat16),
            ((LANES, width), jnp.bfloat16),
            ((count * -(-used // 8) * 8, LANES), jnp.float32),
            ((width, LANES), jnp.bfloat16),
        ],
        [place],
        [ffn_gain.reshape(1, width)],
        [resid_all, chosen, shared_weights],
        [expert_gate, expert_up, expert_down],
    )
    returned = lax.all_to_all(outbound, EP, 0, 0, tiled=True)

    expert_ids, outbound = lax.optimization_barrier((expert_ids, outbound))
    member = jnp.any(
        expert_ids[:, :, None] == jnp.arange(experts, dtype=jnp.int32)[None, None, :], axis=1
    )
    norm_scale = row_scale(resid_own)
    routed_own = (resid_own * norm_scale * ffn_gain).astype(jnp.bfloat16)
    scores = jnp.where(member, jax.nn.sigmoid(matmul(routed_own, router)), 0.0)
    weights = routed_scale * scores / jnp.sum(scores, axis=1, keepdims=True)
    own_member = member.astype(jnp.int32)
    own_slot = jnp.cumsum(own_member, axis=0) - own_member
    by_slot = jnp.concatenate([jnp.where(own_slot == s, weights, 0.0) for s in range(CAP)], axis=1)
    back = returned[:, : CAP * chunks].reshape(count, CAP, width)
    back = jnp.moveaxis(back, 1, 0).reshape(CAP * count, width)
    high, low = split_pair(by_slot)
    routed = matmul(high, back) + matmul(low, back)
    pre = returned[:, CAP * chunks : used].reshape(far, near, rows, 2, units // far)
    pre = jnp.sum(pre.astype(jnp.float32), axis=1).transpose(2, 1, 0, 3).reshape(2, rows, units)
    shared_hidden = (jax.nn.silu(norm_scale * pre[0]) * (norm_scale * pre[1])).astype(jnp.bfloat16)
    layer_out = (resid_own + routed + matmul(shared_hidden, shared_down)).astype(jnp.bfloat16)
    return (layer_out, next_state.reshape(ssm_state.shape), window[:, 1:])


def solution(mesh):
    torus = Mesh(mesh.devices.reshape(mesh.shape["grp"], -1, 2, 2), GRP_EP)
    return jax.shard_map(
        shards,
        mesh=torus,
        in_specs=(
            P(GRP_EP, None),
            P(GRP_EP, None, None),
            P(GRP_EP, None, None, None),
            P(None, EP),
            P(None, EP),
            P(None, EP),
            P(None, EP),
            P(),
            P(),
            P(),
            P(GRP_EP, None),
            P(),
            P(),
            P(),
            P(),
            P(),
            P(None, EP),
            P(),
            P(),
            P(GRP_EP, None),
            P(EP, None, None),
            P(EP, None, None),
            P(EP, None, None),
            P(EP, None),
            P(EP, None),
            P(),
        ),
        out_specs=(P(GRP_EP, None), P(GRP_EP, None, None, None), P(GRP_EP, None, None)),
        check_vma=False,
    )
```

```python
import jax
import jax.numpy as jnp
from jax import lax
from jax.sharding import Mesh
from jax.experimental import pallas as pl
from jax.experimental.pallas import tpu as pltpu
from jax.sharding import PartitionSpec as P

HEAD_DIM = 64
GROUPS = 8
STATE = 128
CAP = 2
EP = ("zh", "zl", "core")
NEAR = ("zl", "core")
GRP_EP = ("grp",) + EP
LANES = 128

epsilon = 1e-06
routed_scale = 2.5


def row_scale(values):
    return lax.rsqrt(jnp.mean(values * values, axis=-1, keepdims=True) + epsilon)


def matmul(left, right):
    return jnp.dot(left, right, preferred_element_type=jnp.float32)


def contract(left, right, left_dim, right_dim):
    return lax.dot_general(
        left, right, (((left_dim,), (right_dim,)), ((), ())), preferred_element_type=jnp.float32
    )


def split_pair(values):
    high = values.astype(jnp.bfloat16)
    low = (values - high.astype(jnp.float32)).astype(jnp.bfloat16)
    return high, low


def near_gather(copies):
    return lax.all_gather(lax.all_to_all(copies, "zh", 0, 0, tiled=True), NEAR)


def kept_in(space, arrays):
    return [pltpu.with_memory_space_constraint(array, space) for array in arrays]


def fast_call(kernel, name, outs, scratch, scalars, fetched, arrays, far=[], remote=[]):
    vmem = pl.BlockSpec(memory_space=pltpu.VMEM)
    smem = pl.BlockSpec(memory_space=pltpu.SMEM)
    hbm = pl.BlockSpec(memory_space=pltpu.HBM)
    specs = [smem] * len(scalars) + [vmem] * (len(fetched) + len(arrays))
    specs += [hbm] * (len(far) + len(remote))
    landing = [pltpu.VMEM(array.shape, array.dtype) for array in far]
    waits = [pltpu.SemaphoreType.DMA((len(far),))] if far else []
    waits += [pltpu.SemaphoreType.DMA((8,))] * len(remote)
    return pl.pallas_call(
        kernel,
        name=name,
        out_shape=tuple(pltpu.VMEM(shape, dtype) for shape, dtype in outs),
        in_specs=specs,
        out_specs=(vmem,) * len(outs),
        scratch_shapes=[pltpu.VMEM(shape, dtype) for shape, dtype in scratch] + landing + waits,
        compiler_params=pltpu.CompilerParams(vmem_limit_bytes=24 * 1024 * 1024),
    )(
        *kept_in(pltpu.HBM, scalars + fetched),
        *kept_in(pltpu.VMEM, arrays),
        *kept_in(pltpu.HBM, far + remote),
    )


def open_kernel(hidden, out, staged):
    rows, width = hidden.shape
    chunks = width // LANES
    values = hidden[...].astype(jnp.float32)
    for k in range(chunks):
        staged[pl.ds(k, rows, stride=chunks), :] = values[:, k * LANES : (k + 1) * LANES]
    mine = staged[...].astype(jnp.bfloat16)
    for z in range(out.shape[0]):
        out[z] = mine


def project_kernel(
    place,
    ids,
    gain,
    gathered,
    gate_hbm,
    input_hbm,
    write_hbm,
    read_hbm,
    message,
    columns,
    flat,
    wide,
    normed,
    staged,
    gate_weights,
    input_weights,
    write_weights,
    read_weights,
    sems,
):
    copies = [
        pltpu.make_async_copy(gate_hbm, gate_weights, sems.at[0]),
        pltpu.make_async_copy(input_hbm, input_weights, sems.at[1]),
        pltpu.make_async_copy(write_hbm, write_weights, sems.at[2]),
        pltpu.make_async_copy(read_hbm, read_weights, sems.at[3]),
    ]
    for copy in copies:
        copy.start()
    near, _, lanes = gathered.shape
    count, lines, _ = message.shape
    far = count // near
    rows = ids.shape[0]
    blocks = gain.shape[1] // lanes
    chunk = rows * blocks
    flat[...] = (
        gathered[:, : far * chunk, :].reshape(count * chunk, lanes).astype(jnp.float32)
    )
    square = jnp.zeros((rows * count, 1), jnp.float32)
    for k in range(blocks):
        for row in range(rows):
            for n in range(near):
                wide[k, pl.ds(row * count + n, far, stride=near), :] = flat[
                    pl.ds(n * far * chunk + row * blocks + k, far, stride=chunk), :
                ]
        part = wide[k]
        square += jnp.sum(part * part, axis=1, keepdims=True)
    scale = lax.rsqrt(square / (blocks * lanes) + epsilon)
    for k in range(blocks):
        span = slice(k * lanes, (k + 1) * lanes)
        normed[:, span] = (wide[k] * scale * gain[:, span]).astype(jnp.bfloat16)
    values = normed[...]
    for copy in copies:
        copy.wait()
    gate_part = jnp.dot(values, gate_weights[...], preferred_element_type=jnp.float32)
    input_part = jnp.dot(values, input_weights[...], preferred_element_type=jnp.float32)
    write_part = contract(values, write_weights[...], 1, 1)
    read_part = contract(values, read_weights[...], 1, 1)

    def of_row(part, row):
        return part[row * count : (row + 1) * count]

    small = lanes - rows * write_part.shape[1]
    expert = lax.broadcasted_iota(jnp.int32, (count, small), 0)
    lane = lax.broadcasted_iota(jnp.int32, (count, small), 1)
    member = jnp.zeros((count, small), jnp.float32)
    for row in range(rows):
        for k in range(ids.shape[1]):
            member = jnp.where((lane == row) & (expert == ids[row, k]), 1.0, member)
    for row in range(rows):
        staged[pl.ds(row, count, stride=lines), :] = of_row(gate_part, row)
        staged[pl.ds(rows + row, count, stride=lines), :] = of_row(input_part, row)
    staged[pl.ds(2 * rows, count, stride=lines), :] = jnp.concatenate(
        [of_row(write_part, row) for row in range(rows)] + [member], axis=1
    )
    staged[pl.ds(2 * rows + 1, count, stride=lines), :] = jnp.concatenate(
        [of_row(read_part, row) for row in range(rows)] + [jnp.zeros_like(member)], axis=1
    )
    message[...] = staged[...].astype(jnp.bfloat16).reshape(count, lines, lanes)

    me = place[0]
    height = columns.shape[0]
    across = jnp.concatenate(
        [wide[me * height // lanes], jnp.zeros((lanes - rows * count, lanes), jnp.float32)], axis=0
    ).T
    columns[...] = jnp.where(me % 2 == 0, across[:height], across[height:])


def output_kernel(gathered, columns, weights_hbm, out, flat, wide, rows, weights, sems):
    copy = pltpu.make_async_copy(weights_hbm, weights, sems.at[0])
    copy.start()
    near, far, chunk, lanes = gathered.shape
    count = near * far
    blocks = weights.shape[1] // lanes
    slabs = chunk // blocks
    flat[...] = gathered[...].reshape(count * chunk, lanes).astype(jnp.float32)
    rows[slabs * count :, :] = jnp.zeros((lanes - slabs * count, blocks * lanes), jnp.bfloat16)
    for k in range(blocks):
        for row in range(slabs):
            for n in range(near):
                wide[k, pl.ds(row * count + n, far, stride=near), :] = flat[
                    pl.ds(n * far * chunk + row * blocks + k, far, stride=chunk), :
                ]
        rows[: slabs * count, k * lanes : (k + 1) * lanes] = wide[k].astype(jnp.bfloat16)
    copy.wait()
    mine = (columns[...] + contract(weights[...], rows[...], 1, 1)).astype(jnp.bfloat16)
    for z in range(out.shape[0]):
        out[z] = mine


def expert_kernel(
    place,
    gain,
    resid,
    chosen,
    gate_hbm,
    up_hbm,
    down_hbm,
    part_hbm,
    out,
    own,
    wide,
    routed,
    shared,
    staged,
    spread,
    gate,
    up,
    down,
    sems,
    part_sems,
):
    near, far, features, lanes = resid.shape
    width = near * far * features
    count, slabs = chosen.shape
    lines = out.shape[1]
    copies = [
        pltpu.make_async_copy(gate_hbm, gate, sems.at[0]),
        pltpu.make_async_copy(up_hbm, up, sems.at[1]),
        pltpu.make_async_copy(down_hbm, down, sems.at[2]),
    ]
    me = place[0]
    first = part_hbm.shape[1] - CAP * near * features
    for n in range(near):
        for s in range(CAP):
            start = pl.multiple_of(first + (s * near + lax.rem(me, near)) * features, features)
            copies.append(
                pltpu.make_async_copy(
                    part_hbm.at[n, pl.ds(start, features)],
                    spread.at[pl.ds(n * features, features), pl.ds(s * LANES, LANES)],
                    part_sems.at[n * CAP + s],
                )
            )
    for copy in copies:
        copy.start()
    square = jnp.zeros((lanes, 1), jnp.float32)
    for z in range(far):
        for pair in range(near // 2):
            block = jnp.concatenate([resid[2 * pair, z], resid[2 * pair + 1, z]], axis=0)
            rows = block.astype(jnp.float32).T
            start = (z * near + 2 * pair) * features
            wide[:, start : start + 2 * features] = rows
            square += jnp.sum(rows * rows, axis=1, keepdims=True)
    scale = lax.rsqrt(square / width + epsilon)
    values = wide[...]
    routed[...] = (values * scale * gain[...]).astype(jnp.bfloat16)
    shared[...] = (values * gain[...]).astype(jnp.bfloat16)

    for row in range(slabs):
        own[row : row + 1, :] = wide[pl.ds(row * count + me, 1), :]
    block = near * features
    for copy in copies[3:]:
        copy.wait()
    start = pl.multiple_of((me // near) * block, block)
    partial = jnp.dot(
        shared[:, pl.ds(start, block)], spread[...], preferred_element_type=jnp.float32
    )
    chunks = width // LANES
    for s in range(CAP):
        for row in range(slabs):
            staged[pl.ds(CAP * chunks + s * slabs + row, count, stride=lines), :] = partial[
                row * count : (row + 1) * count, s * LANES : (s + 1) * LANES
            ]

    copies[0].wait()
    gate_pre = jnp.dot(routed[...], gate[0], preferred_element_type=jnp.float32)
    copies[1].wait()
    up_pre = jnp.dot(routed[...], up[0], preferred_element_type=jnp.float32)
    expert_hidden = (gate_pre / (1.0 + jnp.exp(-gate_pre)) * up_pre).astype(jnp.bfloat16)

    lane = lax.broadcasted_iota(jnp.int32, (count, lanes), 1)
    line = lax.broadcasted_iota(jnp.int32, (count, lanes), 0)
    flags = chosen[...]
    picks = []
    for s in range(CAP):
        pick = jnp.zeros((count, lanes), jnp.float32)
        earlier = jnp.zeros((count, 1), jnp.float32)
        for row in range(slabs):
            flag = flags[:, row : row + 1]
            taken = jnp.where(earlier == float(s), flag, 0.0)
            pick = jnp.where(lane == row * count + line, taken, pick)
            earlier = earlier + flag
        picks.append(pick)
    pick = jnp.concatenate(picks, axis=0).astype(jnp.bfloat16)
    rows = jnp.dot(pick, expert_hidden, preferred_element_type=jnp.float32).astype(jnp.bfloat16)
    copies[2].wait()
    result = jnp.dot(rows, down[0], preferred_element_type=jnp.float32)
    for s in range(CAP):
        for k in range(chunks):
            staged[pl.ds(s * chunks + k, count, stride=lines), :] = result[
                s * count : (s + 1) * count, k * LANES : (k + 1) * LANES
            ]
    used = CAP * (chunks + slabs)
    for k in range(used, lines):
        staged[pl.ds(k, count, stride=lines), :] = jnp.zeros((count, LANES), jnp.float32)
    out[...] = staged[...].astype(jnp.bfloat16).reshape(count, lines, LANES)


def shards(
    hidden,
    conv_window,
    ssm_state,
    gate_proj,
    input_proj,
    write_proj,
    read_proj,
    step_proj,
    step_bias,
    decay_log,
    decay_shift,
    skip_scale,
    conv_taps,
    conv_bias,
    mix_gain,
    group_gain,
    out_proj,
    ffn_gain,
    router,
    expert_ids,
    expert_gate,
    expert_up,
    expert_down,
    shared_gate,
    shared_up,
    shared_down,
):
    rows = hidden.shape[0]
    width = hidden.shape[1]
    index = lax.axis_index(EP)
    count = lax.axis_size(EP)
    near = lax.axis_size(NEAR)
    experts = router.shape[1]
    units = shared_gate.shape[1]
    features = shared_gate.shape[0]

    far = lax.axis_size("zh")
    chunks = width // LANES
    place = index.astype(jnp.int32).reshape(1)
    (opening,) = fast_call(
        open_kernel,
        "open_rows",
        [((far, rows * chunks, LANES), jnp.bfloat16)],
        [((rows * chunks, LANES), jnp.float32)],
        [],
        [hidden],
        [],
    )
    opened = lax.all_to_all(opening, "zh", 0, 0, tiled=True).reshape(-1, LANES)
    later, _ = lax.optimization_barrier(((shared_gate, shared_up), opening))
    blocks = [
        jnp.moveaxis(weights.reshape(features, near, LANES), 1, 0).reshape(-1, LANES)
        for weights in later
    ]
    gathered = lax.all_gather(jnp.concatenate([opened, *blocks], axis=0), NEAR)
    col_width = out_proj.shape[1]
    message, resid_cols = fast_call(
        project_kernel,
        "project_rows",
        [((count, 8, LANES), jnp.bfloat16), ((col_width, LANES), jnp.float32)],
        [
            ((count * rows * chunks, LANES), jnp.float32),
            ((chunks, count * rows, LANES), jnp.float32),
            ((count * rows, width), jnp.bfloat16),
            ((count * 8, LANES), jnp.float32),
        ],
        [place, expert_ids],
        [mix_gain.reshape(1, width)],
        [gathered],
        [gate_proj, input_proj, write_proj.T, read_proj.T],
    )
    pieces = lax.all_to_all(message, EP, 0, 0, tiled=True)

    later = (hidden, conv_window, conv_taps, decay_shift, step_bias, decay_log)
    later, _ = lax.optimization_barrier((later, message))
    hidden_later, conv_window, conv_taps, decay_shift, step_bias, decay_log = later
    hidden_wide = hidden_later.astype(jnp.float32)
    normed_local = (hidden_wide * row_scale(hidden_wide) * mix_gain).astype(jnp.bfloat16)
    step_raw = matmul(normed_local, step_proj)

    gate_rows = jnp.moveaxis(pieces[:, :rows], 0, 1).reshape(rows, -1)
    input_rows = jnp.moveaxis(pieces[:, rows : 2 * rows], 0, 1).reshape(rows, -1)
    tail_width = rows * write_proj.shape[1]
    write_rows, read_rows = (
        jnp.moveaxis(pieces[:, 2 * rows + k, :tail_width].reshape(count, rows, -1), 0, 1).reshape(
            rows, -1
        )
        for k in range(2)
    )
    chosen = pieces[:, 2 * rows, tail_width : tail_width + rows].astype(jnp.float32)

    inner_width = gate_rows.shape[1]
    state_span = GROUPS * STATE
    head_count = step_bias.shape[0]
    per_group = head_count // GROUPS
    fresh_row = jnp.concatenate([input_rows, write_rows, read_rows], axis=1)
    window = jnp.concatenate([conv_window, fresh_row[:, None, :]], axis=1)
    convolved = jax.nn.silu(
        jnp.sum(window.astype(jnp.float32) * conv_taps.astype(jnp.float32)[None], axis=1)
        + conv_bias
    )
    head_input = convolved[:, :inner_width].reshape(rows, GROUPS, per_group, HEAD_DIM)
    write_vec = convolved[:, inner_width : inner_width + state_span].reshape(rows, GROUPS, STATE)
    read_vec = convolved[:, inner_width + state_span :].reshape(rows, GROUPS, STATE)
    step_size = jax.nn.softplus(step_raw + step_bias)
    decay_rate = jnp.exp(decay_shift - step_size * jnp.exp(decay_log)).reshape(
        rows, GROUPS, per_group
    )
    step_group = step_size.reshape(rows, GROUPS, per_group)
    carried = ssm_state.reshape(rows, GROUPS, per_group, HEAD_DIM, STATE)
    next_state = (
        decay_rate[..., None, None] * carried
        + (step_group[..., None] * head_input)[..., None] * write_vec[:, :, None, None, :]
    )
    mixed_out = jnp.einsum("sgepn,sgn->sgep", next_state, read_vec)
    mixed_out = mixed_out + skip_scale.reshape(GROUPS, per_group)[None, :, :, None] * head_input
    mixed_out = mixed_out.reshape(rows, inner_width).astype(jnp.bfloat16)
    gated_out = mixed_out.astype(jnp.float32) * jax.nn.silu(gate_rows.astype(jnp.float32))
    blocks = gated_out.reshape(rows, GROUPS, -1)
    gated_out = ((blocks * row_scale(blocks)).reshape(rows, inner_width) * group_gain).astype(
        jnp.bfloat16
    )

    gated_all = near_gather(
        jnp.broadcast_to(
            gated_out.reshape(1, -1, LANES), (far, rows * inner_width // LANES, LANES)
        )
    )
    (resid_part,) = fast_call(
        output_kernel,
        "output_rows",
        [((far, col_width, LANES), jnp.bfloat16)],
        [
            ((count * rows * inner_width // LANES, LANES), jnp.float32),
            ((inner_width // LANES, rows * count, LANES), jnp.float32),
            ((LANES, inner_width), jnp.bfloat16),
        ],
        [],
        [],
        [gated_all, resid_cols],
        [out_proj.T],
    )
    resid_all = near_gather(resid_part)
    used = CAP * (chunks + rows)
    outbound, resid_own = fast_call(
        expert_kernel,
        "expert_rows",
        [((count, -(-used // 8) * 8, LANES), jnp.bfloat16), ((rows, width), jnp.float32)],
        [
            ((LANES, width), jnp.float32),
            ((LANES, width), jnp.bfloat16),
            ((LANES, width), jnp.bfloat16),
            ((count * -(-used // 8) * 8, LANES), jnp.float32),
            ((near * features, CAP * LANES), jnp.bfloat16),
        ],
        [place],
        [ffn_gain.reshape(1, width)],
        [resid_all, chosen],
        [expert_gate, expert_up, expert_down],
        [gathered],
    )
    returned = lax.all_to_all(outbound, EP, 0, 0, tiled=True)

    expert_ids, outbound = lax.optimization_barrier((expert_ids, outbound))
    member = jnp.any(
        expert_ids[:, :, None] == jnp.arange(experts, dtype=jnp.int32)[None, None, :], axis=1
    )
    norm_scale = row_scale(resid_own)
    routed_own = (resid_own * norm_scale * ffn_gain).astype(jnp.bfloat16)
    scores = jnp.where(member, jax.nn.sigmoid(matmul(routed_own, router)), 0.0)
    weights = routed_scale * scores / jnp.sum(scores, axis=1, keepdims=True)
    own_member = member.astype(jnp.int32)
    own_slot = jnp.cumsum(own_member, axis=0) - own_member
    by_slot = jnp.concatenate([jnp.where(own_slot == s, weights, 0.0) for s in range(CAP)], axis=1)
    back = returned[:, : CAP * chunks].reshape(count, CAP, width)
    back = jnp.moveaxis(back, 1, 0).reshape(CAP * count, width)
    high, low = split_pair(by_slot)
    routed = matmul(high, back) + matmul(low, back)
    pre = returned[:, CAP * chunks : used].reshape(far, near, 2, rows, units // near)
    pre = jnp.sum(pre.astype(jnp.float32), axis=0).transpose(1, 2, 0, 3).reshape(2, rows, units)
    shared_hidden = (jax.nn.silu(norm_scale * pre[0]) * (norm_scale * pre[1])).astype(jnp.bfloat16)
    layer_out = (resid_own + routed + matmul(shared_hidden, shared_down)).astype(jnp.bfloat16)
    return (layer_out, next_state.reshape(ssm_state.shape), window[:, 1:])


def solution(mesh):
    torus = Mesh(mesh.devices.reshape(mesh.shape["grp"], -1, 2, 2), GRP_EP)
    return jax.shard_map(
        shards,
        mesh=torus,
        in_specs=(
            P(GRP_EP, None),
            P(GRP_EP, None, None),
            P(GRP_EP, None, None, None),
            P(None, EP),
            P(None, EP),
            P(None, EP),
            P(None, EP),
            P(),
            P(),
            P(),
            P(GRP_EP, None),
            P(),
            P(),
            P(),
            P(),
            P(),
            P(None, EP),
            P(),
            P(),
            P(GRP_EP, None),
            P(EP, None, None),
            P(EP, None, None),
            P(EP, None, None),
            P(EP, None),
            P(EP, None),
            P(),
        ),
        out_specs=(P(GRP_EP, None), P(GRP_EP, None, None, None), P(GRP_EP, None, None)),
        check_vma=False,
    )
```

```python
import jax
import jax.numpy as jnp
from jax import lax
from jax.sharding import Mesh
from jax.experimental import pallas as pl
from jax.experimental.pallas import tpu as pltpu
from jax.sharding import PartitionSpec as P

HEAD_DIM = 64
GROUPS = 8
STATE = 128
CAP = 2
EP = ("zh", "zl", "core")
NEAR = ("zl", "core")
GRP_EP = ("grp",) + EP
LANES = 128

epsilon = 1e-06
routed_scale = 2.5


def row_scale(values):
    return lax.rsqrt(jnp.mean(values * values, axis=-1, keepdims=True) + epsilon)


def matmul(left, right):
    return jnp.dot(left, right, preferred_element_type=jnp.float32)


def contract(left, right, left_dim, right_dim):
    return lax.dot_general(
        left, right, (((left_dim,), (right_dim,)), ((), ())), preferred_element_type=jnp.float32
    )


def split_pair(values):
    high = values.astype(jnp.bfloat16)
    low = (values - high.astype(jnp.float32)).astype(jnp.bfloat16)
    return high, low


def near_gather(copies):
    return lax.all_gather(lax.all_to_all(copies, "zh", 0, 0, tiled=True), NEAR)


def kept_in(space, arrays):
    return [pltpu.with_memory_space_constraint(array, space) for array in arrays]


def fast_call(kernel, name, outs, scratch, scalars, fetched, arrays, far=[], remote=[]):
    vmem = pl.BlockSpec(memory_space=pltpu.VMEM)
    smem = pl.BlockSpec(memory_space=pltpu.SMEM)
    hbm = pl.BlockSpec(memory_space=pltpu.HBM)
    specs = [smem] * len(scalars) + [vmem] * (len(fetched) + len(arrays))
    specs += [hbm] * (len(far) + len(remote))
    landing = [pltpu.VMEM(array.shape, array.dtype) for array in far]
    waits = [pltpu.SemaphoreType.DMA((4,))] if far else []
    waits += [pltpu.SemaphoreType.DMA((8,))] * len(remote)
    return pl.pallas_call(
        kernel,
        name=name,
        out_shape=tuple(pltpu.VMEM(shape, dtype) for shape, dtype in outs),
        in_specs=specs,
        out_specs=(vmem,) * len(outs),
        scratch_shapes=[pltpu.VMEM(shape, dtype) for shape, dtype in scratch] + landing + waits,
        compiler_params=pltpu.CompilerParams(vmem_limit_bytes=24 * 1024 * 1024),
    )(
        *kept_in(pltpu.HBM, scalars + fetched),
        *kept_in(pltpu.VMEM, arrays),
        *kept_in(pltpu.HBM, far + remote),
    )


def open_kernel(hidden, out, staged):
    rows, width = hidden.shape
    chunks = width // LANES
    values = hidden[...].astype(jnp.float32)
    for k in range(chunks):
        staged[pl.ds(k, rows, stride=chunks), :] = values[:, k * LANES : (k + 1) * LANES]
    mine = staged[...].astype(jnp.bfloat16)
    for z in range(out.shape[0]):
        out[z] = mine


def project_kernel(
    place,
    ids,
    gain,
    gathered,
    gate_hbm,
    input_hbm,
    write_hbm,
    read_hbm,
    message,
    columns,
    flat,
    wide,
    normed,
    staged,
    gate_weights,
    input_weights,
    write_weights,
    read_weights,
    sems,
):
    copies = [
        pltpu.make_async_copy(gate_hbm, gate_weights, sems.at[0]),
        pltpu.make_async_copy(input_hbm, input_weights, sems.at[1]),
        pltpu.make_async_copy(write_hbm, write_weights, sems.at[2]),
        pltpu.make_async_copy(read_hbm, read_weights, sems.at[3]),
    ]
    for copy in copies:
        copy.start()
    near, _, lanes = gathered.shape
    count, lines, _ = message.shape
    far = count // near
    rows = ids.shape[0]
    blocks = gain.shape[1] // lanes
    chunk = rows * blocks
    flat[...] = (
        gathered[:, : far * chunk, :].reshape(count * chunk, lanes).astype(jnp.float32)
    )
    square = jnp.zeros((rows * count, 1), jnp.float32)
    for k in range(blocks):
        for row in range(rows):
            for n in range(near):
                wide[k, pl.ds(row * count + n, far, stride=near), :] = flat[
                    pl.ds(n * far * chunk + row * blocks + k, far, stride=chunk), :
                ]
        part = wide[k]
        square += jnp.sum(part * part, axis=1, keepdims=True)
    scale = lax.rsqrt(square / (blocks * lanes) + epsilon)
    for k in range(blocks):
        span = slice(k * lanes, (k + 1) * lanes)
        normed[:, span] = (wide[k] * scale * gain[:, span]).astype(jnp.bfloat16)
    values = normed[...]
    for copy in copies:
        copy.wait()
    gate_part = jnp.dot(values, gate_weights[...], preferred_element_type=jnp.float32)
    input_part = jnp.dot(values, input_weights[...], preferred_element_type=jnp.float32)
    write_part = contract(values, write_weights[...], 1, 1)
    read_part = contract(values, read_weights[...], 1, 1)

    def of_row(part, row):
        return part[row * count : (row + 1) * count]

    small = lanes - rows * write_part.shape[1]
    expert = lax.broadcasted_iota(jnp.int32, (count, small), 0)
    lane = lax.broadcasted_iota(jnp.int32, (count, small), 1)
    member = jnp.zeros((count, small), jnp.float32)
    for row in range(rows):
        for k in range(ids.shape[1]):
            member = jnp.where((lane == row) & (expert == ids[row, k]), 1.0, member)
    for row in range(rows):
        staged[pl.ds(row, count, stride=lines), :] = of_row(gate_part, row)
        staged[pl.ds(rows + row, count, stride=lines), :] = of_row(input_part, row)
    staged[pl.ds(2 * rows, count, stride=lines), :] = jnp.concatenate(
        [of_row(write_part, row) for row in range(rows)] + [member], axis=1
    )
    staged[pl.ds(2 * rows + 1, count, stride=lines), :] = jnp.concatenate(
        [of_row(read_part, row) for row in range(rows)] + [jnp.zeros_like(member)], axis=1
    )
    message[...] = staged[...].astype(jnp.bfloat16).reshape(count, lines, lanes)

    me = place[0]
    height = columns.shape[0]
    across = jnp.concatenate(
        [wide[me * height // lanes], jnp.zeros((lanes - rows * count, lanes), jnp.float32)], axis=0
    ).T
    columns[...] = jnp.where(me % 2 == 0, across[:height], across[height:])


def mixer_kernel(
    gain, bias, heads, window, taps, pieces, state_hbm, out, fresh, fed, written, named, flat, state, sems
):
    far = out.shape[0]
    slabs = fresh.shape[0]
    past = taps.shape[0] - 1
    count, lines, lanes = pieces.shape
    groups = written.shape[1]
    blocks = fed.shape[1]
    share = blocks // groups
    quarter = lanes // share
    pair = lanes // state.shape[2]
    copies = [
        pltpu.make_async_copy(state_hbm.at[row], state.at[row], sems.at[row])
        for row in range(slabs)
    ]
    for copy in copies:
        copy.start()
    flat[...] = pieces[...].reshape(count * lines, lanes).astype(jnp.float32)
    named[...] = flat[pl.ds(2 * slabs, count, stride=lines), :]
    line = lax.broadcasted_iota(jnp.int32, (blocks, lanes), 0)
    lane = lax.broadcasted_iota(jnp.int32, (blocks, lanes), 1)
    lane_of = lax.broadcasted_iota(jnp.int32, (groups, lanes), 1)
    wide_lane = lax.broadcasted_iota(jnp.int32, (lanes, lanes), 1)
    even = heads[pl.ds(0, blocks, stride=pair), :]
    odd = heads[pl.ds(1, blocks, stride=pair), :]

    def per_head(column):
        return jnp.where(
            lane < lanes // 2, even[:, column : column + 1], odd[:, column : column + 1]
        )

    def by_group(values):
        spread = jnp.zeros((blocks, lanes), jnp.float32)
        for g in range(groups):
            spread = jnp.where(line // share == g, values(g), spread)
        return spread

    skip = per_head(2 * slabs)
    for row in range(slabs):
        gate = flat[pl.ds(row, count, stride=lines), :]
        vectors = []
        for kind in range(2):
            vector = jnp.zeros((groups, lanes), jnp.float32)
            for q in range(share):
                part = flat[pl.ds(q * lines + 2 * slabs + kind, groups, stride=share * lines), :]
                shift = (q - row) * quarter % lanes
                part = pltpu.roll(part, shift, 1) if shift else part
                vector = jnp.where(lane_of // quarter == q, part, vector)
            vectors.append(vector)
        newest = jnp.concatenate(
            [flat[pl.ds(slabs + row, count, stride=lines), :]] + vectors, axis=0
        )
        fresh[row] = newest.astype(jnp.bfloat16)
        taken = newest * taps[past].astype(jnp.float32)
        for t in range(past):
            taken += window[row * past + t].astype(jnp.float32) * taps[t].astype(jnp.float32)
        taken += bias[...]
        convolved = taken / (1.0 + jnp.exp(-taken))
        head_input = convolved[:blocks]
        write = convolved[blocks : blocks + groups]
        read = convolved[blocks + groups :]
        steps = per_head(row) * head_input
        fed[row] = steps
        written[row] = write
        overlap = jnp.sum(write * read, axis=1, keepdims=True)
        direct = by_group(lambda g: overlap[g : g + 1])
        copies[row].wait()
        columns = jnp.zeros((lanes, lanes), jnp.float32)
        for j in range(blocks):
            block = state[row, pair * j : pair * (j + 1)].reshape(lanes, lanes)
            g = j // share
            total = jnp.sum(block * read[g : g + 1], axis=1, keepdims=True)
            columns = jnp.where(wide_lane == j, total, columns)
        mixed = per_head(slabs + row) * columns.T[:blocks] + steps * direct + skip * head_input
        mixed = mixed.astype(jnp.bfloat16).astype(jnp.float32)
        gated = mixed * (gate / (1.0 + jnp.exp(-gate)))
        square = jnp.sum(gated * gated, axis=1, keepdims=True)
        total = by_group(
            lambda g: jnp.sum(square[g * share : (g + 1) * share], axis=0, keepdims=True)
        )
        scale = lax.rsqrt(total / (share * lanes) + epsilon)
        result = (gated * scale * gain[...]).astype(jnp.bfloat16)
        for z in range(far):
            out[z, row * blocks : (row + 1) * blocks] = result


def output_kernel(gathered, columns, weights_hbm, out, flat, wide, rows, weights, sems):
    copy = pltpu.make_async_copy(weights_hbm, weights, sems.at[0])
    copy.start()
    near, far, chunk, lanes = gathered.shape
    count = near * far
    blocks = weights.shape[1] // lanes
    slabs = chunk // blocks
    flat[...] = gathered[...].reshape(count * chunk, lanes).astype(jnp.float32)
    rows[slabs * count :, :] = jnp.zeros((lanes - slabs * count, blocks * lanes), jnp.bfloat16)
    for k in range(blocks):
        for row in range(slabs):
            for n in range(near):
                wide[k, pl.ds(row * count + n, far, stride=near), :] = flat[
                    pl.ds(n * far * chunk + row * blocks + k, far, stride=chunk), :
                ]
        rows[: slabs * count, k * lanes : (k + 1) * lanes] = wide[k].astype(jnp.bfloat16)
    copy.wait()
    mine = (columns[...] + contract(weights[...], rows[...], 1, 1)).astype(jnp.bfloat16)
    for z in range(out.shape[0]):
        out[z] = mine


def expert_kernel(
    place,
    gain,
    resid,
    chosen,
    gate_hbm,
    up_hbm,
    down_hbm,
    part_hbm,
    out,
    own,
    wide,
    routed,
    shared,
    staged,
    spread,
    gate,
    up,
    down,
    sems,
    part_sems,
):
    near, far, features, lanes = resid.shape
    width = near * far * features
    count = chosen.shape[0]
    slabs = own.shape[0]
    lines = out.shape[1]
    copies = [
        pltpu.make_async_copy(gate_hbm, gate, sems.at[0]),
        pltpu.make_async_copy(up_hbm, up, sems.at[1]),
        pltpu.make_async_copy(down_hbm, down, sems.at[2]),
    ]
    me = place[0]
    first = part_hbm.shape[1] - CAP * near * features
    for n in range(near):
        for s in range(CAP):
            start = pl.multiple_of(first + (s * near + lax.rem(me, near)) * features, features)
            copies.append(
                pltpu.make_async_copy(
                    part_hbm.at[n, pl.ds(start, features)],
                    spread.at[pl.ds(n * features, features), pl.ds(s * LANES, LANES)],
                    part_sems.at[n * CAP + s],
                )
            )
    for copy in copies:
        copy.start()
    square = jnp.zeros((lanes, 1), jnp.float32)
    for z in range(far):
        for pair in range(near // 2):
            block = jnp.concatenate([resid[2 * pair, z], resid[2 * pair + 1, z]], axis=0)
            rows = block.astype(jnp.float32).T
            start = (z * near + 2 * pair) * features
            wide[:, start : start + 2 * features] = rows
            square += jnp.sum(rows * rows, axis=1, keepdims=True)
    scale = lax.rsqrt(square / width + epsilon)
    values = wide[...]
    routed[...] = (values * scale * gain[...]).astype(jnp.bfloat16)
    shared[...] = (values * gain[...]).astype(jnp.bfloat16)

    for row in range(slabs):
        own[row : row + 1, :] = wide[pl.ds(row * count + me, 1), :]
    block = near * features
    for copy in copies[3:]:
        copy.wait()
    start = pl.multiple_of((me // near) * block, block)
    partial = jnp.dot(
        shared[:, pl.ds(start, block)], spread[...], preferred_element_type=jnp.float32
    )
    chunks = width // LANES
    for s in range(CAP):
        for row in range(slabs):
            staged[pl.ds(CAP * chunks + s * slabs + row, count, stride=lines), :] = partial[
                row * count : (row + 1) * count, s * LANES : (s + 1) * LANES
            ]

    copies[0].wait()
    gate_pre = jnp.dot(routed[...], gate[0], preferred_element_type=jnp.float32)
    copies[1].wait()
    up_pre = jnp.dot(routed[...], up[0], preferred_element_type=jnp.float32)
    expert_hidden = (gate_pre / (1.0 + jnp.exp(-gate_pre)) * up_pre).astype(jnp.bfloat16)

    lane = lax.broadcasted_iota(jnp.int32, (count, lanes), 1)
    line = lax.broadcasted_iota(jnp.int32, (count, lanes), 0)
    flags = chosen[:, slabs * (LANES // (slabs + 1)) :]
    picks = []
    for s in range(CAP):
        pick = jnp.zeros((count, lanes), jnp.float32)
        earlier = jnp.zeros((count, 1), jnp.float32)
        for row in range(slabs):
            flag = flags[:, row : row + 1]
            taken = jnp.where(earlier == float(s), flag, 0.0)
            pick = jnp.where(lane == row * count + line, taken, pick)
            earlier = earlier + flag
        picks.append(pick)
    pick = jnp.concatenate(picks, axis=0).astype(jnp.bfloat16)
    rows = jnp.dot(pick, expert_hidden, preferred_element_type=jnp.float32).astype(jnp.bfloat16)
    copies[2].wait()
    result = jnp.dot(rows, down[0], preferred_element_type=jnp.float32)
    for s in range(CAP):
        for k in range(chunks):
            staged[pl.ds(s * chunks + k, count, stride=lines), :] = result[
                s * count : (s + 1) * count, k * LANES : (k + 1) * LANES
            ]
    used = CAP * (chunks + slabs)
    for k in range(used, lines):
        staged[pl.ds(k, count, stride=lines), :] = jnp.zeros((count, LANES), jnp.float32)
    out[...] = staged[...].astype(jnp.bfloat16).reshape(count, lines, LANES)


def shards(
    hidden,
    conv_window,
    ssm_state,
    gate_proj,
    input_proj,
    write_proj,
    read_proj,
    step_proj,
    step_bias,
    decay_log,
    decay_shift,
    skip_scale,
    conv_taps,
    conv_bias,
    mix_gain,
    group_gain,
    out_proj,
    ffn_gain,
    router,
    expert_ids,
    expert_gate,
    expert_up,
    expert_down,
    shared_gate,
    shared_up,
    shared_down,
):
    rows = hidden.shape[0]
    width = hidden.shape[1]
    index = lax.axis_index(EP)
    count = lax.axis_size(EP)
    near = lax.axis_size(NEAR)
    experts = router.shape[1]
    units = shared_gate.shape[1]
    features = shared_gate.shape[0]

    far = lax.axis_size("zh")
    chunks = width // LANES
    place = index.astype(jnp.int32).reshape(1)
    (opening,) = fast_call(
        open_kernel,
        "open_rows",
        [((far, rows * chunks, LANES), jnp.bfloat16)],
        [((rows * chunks, LANES), jnp.float32)],
        [],
        [hidden],
        [],
    )
    opened = lax.all_to_all(opening, "zh", 0, 0, tiled=True).reshape(-1, LANES)
    later = (shared_gate, shared_up, conv_window, conv_taps, conv_bias, group_gain)
    later, _ = lax.optimization_barrier((later, opening))
    blocks = [
        jnp.moveaxis(weights.reshape(features, near, LANES), 1, 0).reshape(-1, LANES)
        for weights in later[:2]
    ]
    span = conv_bias.shape[0] // LANES
    window_blocks = later[2].reshape(-1, span, LANES)
    taps_blocks = later[3].reshape(-1, span, LANES)
    bias_blocks = later[4].reshape(-1, LANES)
    group_gain = later[5].reshape(-1, LANES)
    gathered = lax.all_gather(jnp.concatenate([opened, *blocks], axis=0), NEAR)
    col_width = out_proj.shape[1]
    message, resid_cols = fast_call(
        project_kernel,
        "project_rows",
        [((count, 8, LANES), jnp.bfloat16), ((col_width, LANES), jnp.float32)],
        [
            ((count * rows * chunks, LANES), jnp.float32),
            ((chunks, count * rows, LANES), jnp.float32),
            ((count * rows, width), jnp.bfloat16),
            ((count * 8, LANES), jnp.float32),
        ],
        [place, expert_ids],
        [mix_gain.reshape(1, width)],
        [gathered],
        [gate_proj, input_proj, write_proj.T, read_proj.T],
    )
    pieces = lax.all_to_all(message, EP, 0, 0, tiled=True)

    later = (hidden, decay_shift, step_bias, decay_log, skip_scale)
    later, _ = lax.optimization_barrier((later, message))
    hidden_later, decay_shift, step_bias, decay_log, skip_scale = later
    hidden_wide = hidden_later.astype(jnp.float32)
    normed_local = (hidden_wide * row_scale(hidden_wide) * mix_gain).astype(jnp.bfloat16)
    step_raw = matmul(normed_local, step_proj)

    inner_width = out_proj.shape[0]
    blocks = inner_width // LANES
    step_size = jax.nn.softplus(step_raw + step_bias)
    decay_rate = jnp.exp(decay_shift - step_size * jnp.exp(decay_log))
    heads = jnp.concatenate([step_size, decay_rate, skip_scale[None]], axis=0)
    heads = jnp.pad(heads, ((0, LANES - heads.shape[0]), (0, 0))).T
    gated_rows, fresh, fed, write_vec, chosen = fast_call(
        mixer_kernel,
        "mix_rows",
        [
            ((far, rows * blocks, LANES), jnp.bfloat16),
            ((rows, span, LANES), jnp.bfloat16),
            ((rows, blocks, LANES), jnp.float32),
            ((rows, GROUPS, STATE), jnp.float32),
            ((count, LANES), jnp.float32),
        ],
        [((count * 8, LANES), jnp.float32)],
        [],
        [group_gain, bias_blocks],
        [heads, window_blocks, taps_blocks, pieces],
        [ssm_state],
    )
    gated_all = near_gather(gated_rows)
    (resid_part,) = fast_call(
        output_kernel,
        "output_rows",
        [((far, col_width, LANES), jnp.bfloat16)],
        [
            ((count * rows * inner_width // LANES, LANES), jnp.float32),
            ((inner_width // LANES, rows * count, LANES), jnp.float32),
            ((LANES, inner_width), jnp.bfloat16),
        ],
        [],
        [],
        [gated_all, resid_cols],
        [out_proj.T],
    )
    resid_all = near_gather(resid_part)
    used = CAP * (chunks + rows)
    outbound, resid_own = fast_call(
        expert_kernel,
        "expert_rows",
        [((count, -(-used // 8) * 8, LANES), jnp.bfloat16), ((rows, width), jnp.float32)],
        [
            ((LANES, width), jnp.float32),
            ((LANES, width), jnp.bfloat16),
            ((LANES, width), jnp.bfloat16),
            ((count * -(-used // 8) * 8, LANES), jnp.float32),
            ((near * features, CAP * LANES), jnp.bfloat16),
        ],
        [place],
        [ffn_gain.reshape(1, width)],
        [resid_all, chosen],
        [expert_gate, expert_up, expert_down],
        [gathered],
    )
    returned = lax.all_to_all(outbound, EP, 0, 0, tiled=True)

    later = (expert_ids, conv_window, fresh, fed, write_vec, decay_rate)
    later, _ = lax.optimization_barrier((later, outbound))
    expert_ids, conv_window, fresh, fed, write_vec, decay_rate = later
    next_window = jnp.concatenate([conv_window[:, 1:], fresh.reshape(rows, 1, -1)], axis=1)
    per_group = step_size.shape[1] // GROUPS
    next_state = (
        decay_rate[:, :, None, None] * ssm_state
        + fed.reshape(rows, -1, HEAD_DIM)[..., None]
        * jnp.repeat(write_vec, per_group, axis=1)[:, :, None, :]
    )
    member = jnp.any(
        expert_ids[:, :, None] == jnp.arange(experts, dtype=jnp.int32)[None, None, :], axis=1
    )
    norm_scale = row_scale(resid_own)
    routed_own = (resid_own * norm_scale * ffn_gain).astype(jnp.bfloat16)
    scores = jnp.where(member, jax.nn.sigmoid(matmul(routed_own, router)), 0.0)
    weights = routed_scale * scores / jnp.sum(scores, axis=1, keepdims=True)
    own_member = member.astype(jnp.int32)
    own_slot = jnp.cumsum(own_member, axis=0) - own_member
    by_slot = jnp.concatenate([jnp.where(own_slot == s, weights, 0.0) for s in range(CAP)], axis=1)
    back = returned[:, : CAP * chunks].reshape(count, CAP, width)
    back = jnp.moveaxis(back, 1, 0).reshape(CAP * count, width)
    high, low = split_pair(by_slot)
    routed = matmul(high, back) + matmul(low, back)
    pre = returned[:, CAP * chunks : used].reshape(far, near, 2, rows, units // near)
    pre = jnp.sum(pre.astype(jnp.float32), axis=0).transpose(1, 2, 0, 3).reshape(2, rows, units)
    shared_hidden = (jax.nn.silu(norm_scale * pre[0]) * (norm_scale * pre[1])).astype(jnp.bfloat16)
    layer_out = (resid_own + routed + matmul(shared_hidden, shared_down)).astype(jnp.bfloat16)
    return (layer_out, next_state, next_window)


def solution(mesh):
    torus = Mesh(mesh.devices.reshape(mesh.shape["grp"], -1, 2, 2), GRP_EP)
    return jax.shard_map(
        shards,
        mesh=torus,
        in_specs=(
            P(GRP_EP, None),
            P(GRP_EP, None, None),
            P(GRP_EP, None, None, None),
            P(None, EP),
            P(None, EP),
            P(None, EP),
            P(None, EP),
            P(),
            P(),
            P(),
            P(GRP_EP, None),
            P(),
            P(),
            P(),
            P(),
            P(),
            P(None, EP),
            P(),
            P(),
            P(GRP_EP, None),
            P(EP, None, None),
            P(EP, None, None),
            P(EP, None, None),
            P(EP, None),
            P(EP, None),
            P(),
        ),
        out_specs=(P(GRP_EP, None), P(GRP_EP, None, None, None), P(GRP_EP, None, None)),
        check_vma=False,
    )
```

```python
import jax
import jax.numpy as jnp
from jax import lax
from jax.sharding import Mesh
from jax.experimental import pallas as pl
from jax.experimental.pallas import tpu as pltpu
from jax.sharding import PartitionSpec as P

HEAD_DIM = 64
GROUPS = 8
STATE = 128
CAP = 2
EP = ("zh", "zl", "core")
NEAR = ("zl", "core")
GRP_EP = ("grp",) + EP
LANES = 128

epsilon = 1e-06
routed_scale = 2.5


def row_scale(values):
    return lax.rsqrt(jnp.mean(values * values, axis=-1, keepdims=True) + epsilon)


def matmul(left, right):
    return jnp.dot(left, right, preferred_element_type=jnp.float32)


def contract(left, right, left_dim, right_dim):
    return lax.dot_general(
        left, right, (((left_dim,), (right_dim,)), ((), ())), preferred_element_type=jnp.float32
    )


def split_pair(values):
    high = values.astype(jnp.bfloat16)
    low = (values - high.astype(jnp.float32)).astype(jnp.bfloat16)
    return high, low


def near_gather(copies):
    return lax.all_gather(lax.all_to_all(copies, "zh", 0, 0, tiled=True), NEAR)


def kept_in(space, arrays):
    return [pltpu.with_memory_space_constraint(array, space) for array in arrays]


class Late:
    def __init__(self, source, landing, sem):
        self.copy = pltpu.make_async_copy(source, landing, sem)
        self.landing = landing
        self.shape = landing.shape
        self.here = False

    def __getitem__(self, place):
        if not self.here:
            self.copy.wait()
            self.here = True
        return self.landing[place]


def fast_call(kernel, name, outs, scratch, scalars, fetched, arrays, far=[], remote=[]):
    vmem = pl.BlockSpec(memory_space=pltpu.VMEM)
    hbm = pl.BlockSpec(memory_space=pltpu.HBM)
    late = len(scalars) + len(fetched)
    specs = [hbm] * late + [vmem] * len(arrays) + [hbm] * (len(far) + len(remote))
    landing = [pltpu.VMEM(array.shape, array.dtype) for array in far]
    waits = [pltpu.SemaphoreType.DMA((4,))] if far else []
    waits += [pltpu.SemaphoreType.DMA((8,))] * len(remote)
    ends = [pltpu.SMEM(array.shape, array.dtype) for array in scalars]
    ends += [pltpu.VMEM(array.shape, array.dtype) for array in fetched]
    ends += [pltpu.SemaphoreType.DMA((late,))] if late else []

    def body(*refs):
        if not late:
            return kernel(*refs)
        sems = refs[-1]
        operands = [
            Late(refs[k], refs[len(refs) - 1 - late + k], sems.at[k]) for k in range(late)
        ]
        for operand in operands:
            operand.copy.start()
        kernel(*operands, *refs[late : len(refs) - 1 - late])
        assert all(operand.here for operand in operands)

    return pl.pallas_call(
        body,
        name=name,
        out_shape=tuple(pltpu.VMEM(shape, dtype) for shape, dtype in outs),
        in_specs=specs,
        out_specs=(vmem,) * len(outs),
        scratch_shapes=[pltpu.VMEM(shape, dtype) for shape, dtype in scratch]
        + landing
        + waits
        + ends,
        compiler_params=pltpu.CompilerParams(vmem_limit_bytes=24 * 1024 * 1024),
    )(
        *kept_in(pltpu.HBM, scalars + fetched),
        *kept_in(pltpu.VMEM, arrays),
        *kept_in(pltpu.HBM, far + remote),
    )


def open_kernel(hidden, out, staged):
    rows, width = hidden.shape
    chunks = width // LANES
    values = hidden[...].astype(jnp.float32)
    for k in range(chunks):
        staged[pl.ds(k, rows, stride=chunks), :] = values[:, k * LANES : (k + 1) * LANES]
    mine = staged[...].astype(jnp.bfloat16)
    for z in range(out.shape[0]):
        out[z] = mine


def project_kernel(
    place,
    ids,
    gain,
    gathered,
    gate_hbm,
    input_hbm,
    write_hbm,
    read_hbm,
    message,
    columns,
    flat,
    wide,
    normed,
    staged,
    gate_weights,
    input_weights,
    write_weights,
    read_weights,
    sems,
):
    copies = [
        pltpu.make_async_copy(gate_hbm, gate_weights, sems.at[0]),
        pltpu.make_async_copy(input_hbm, input_weights, sems.at[1]),
        pltpu.make_async_copy(write_hbm, write_weights, sems.at[2]),
        pltpu.make_async_copy(read_hbm, read_weights, sems.at[3]),
    ]
    for copy in copies:
        copy.start()
    near, _, lanes = gathered.shape
    count, lines, _ = message.shape
    far = count // near
    rows = ids.shape[0]
    blocks = gain.shape[1] // lanes
    chunk = rows * blocks
    flat[...] = (
        gathered[:, : far * chunk, :].reshape(count * chunk, lanes).astype(jnp.float32)
    )
    square = jnp.zeros((rows * count, 1), jnp.float32)
    for k in range(blocks):
        for row in range(rows):
            for n in range(near):
                wide[k, pl.ds(row * count + n, far, stride=near), :] = flat[
                    pl.ds(n * far * chunk + row * blocks + k, far, stride=chunk), :
                ]
        part = wide[k]
        square += jnp.sum(part * part, axis=1, keepdims=True)
    scale = lax.rsqrt(square / (blocks * lanes) + epsilon)
    for k in range(blocks):
        span = slice(k * lanes, (k + 1) * lanes)
        normed[:, span] = (wide[k] * scale * gain[:, span]).astype(jnp.bfloat16)
    values = normed[...]
    for copy in copies:
        copy.wait()
    gate_part = jnp.dot(values, gate_weights[...], preferred_element_type=jnp.float32)
    input_part = jnp.dot(values, input_weights[...], preferred_element_type=jnp.float32)
    write_part = contract(values, write_weights[...], 1, 1)
    read_part = contract(values, read_weights[...], 1, 1)

    def of_row(part, row):
        return part[row * count : (row + 1) * count]

    small = lanes - rows * write_part.shape[1]
    expert = lax.broadcasted_iota(jnp.int32, (count, small), 0)
    lane = lax.broadcasted_iota(jnp.int32, (count, small), 1)
    member = jnp.zeros((count, small), jnp.float32)
    for row in range(rows):
        for k in range(ids.shape[1]):
            member = jnp.where((lane == row) & (expert == ids[row, k]), 1.0, member)
    for row in range(rows):
        staged[pl.ds(row, count, stride=lines), :] = of_row(gate_part, row)
        staged[pl.ds(rows + row, count, stride=lines), :] = of_row(input_part, row)
    staged[pl.ds(2 * rows, count, stride=lines), :] = jnp.concatenate(
        [of_row(write_part, row) for row in range(rows)] + [member], axis=1
    )
    staged[pl.ds(2 * rows + 1, count, stride=lines), :] = jnp.concatenate(
        [of_row(read_part, row) for row in range(rows)] + [jnp.zeros_like(member)], axis=1
    )
    message[...] = staged[...].astype(jnp.bfloat16).reshape(count, lines, lanes)

    me = place[0]
    height = columns.shape[0]
    across = jnp.concatenate(
        [wide[me * height // lanes], jnp.zeros((lanes - rows * count, lanes), jnp.float32)], axis=0
    ).T
    columns[...] = jnp.where(me % 2 == 0, across[:height], across[height:])


def mixer_kernel(
    gain, bias, heads, window, taps, pieces, state_hbm, out, fresh, fed, written, named, flat, state, sems
):
    far = out.shape[0]
    slabs = fresh.shape[0]
    past = taps.shape[0] - 1
    count, lines, lanes = pieces.shape
    groups = written.shape[1]
    blocks = fed.shape[1]
    share = blocks // groups
    quarter = lanes // share
    pair = lanes // state.shape[2]
    copies = [
        pltpu.make_async_copy(state_hbm.at[row], state.at[row], sems.at[row])
        for row in range(slabs)
    ]
    for copy in copies:
        copy.start()
    flat[...] = pieces[...].reshape(count * lines, lanes).astype(jnp.float32)
    named[...] = flat[pl.ds(2 * slabs, count, stride=lines), :]
    line = lax.broadcasted_iota(jnp.int32, (blocks, lanes), 0)
    lane = lax.broadcasted_iota(jnp.int32, (blocks, lanes), 1)
    lane_of = lax.broadcasted_iota(jnp.int32, (groups, lanes), 1)
    wide_lane = lax.broadcasted_iota(jnp.int32, (lanes, lanes), 1)
    even = heads[pl.ds(0, blocks, stride=pair), :]
    odd = heads[pl.ds(1, blocks, stride=pair), :]

    def per_head(column):
        return jnp.where(
            lane < lanes // 2, even[:, column : column + 1], odd[:, column : column + 1]
        )

    def by_group(values):
        spread = jnp.zeros((blocks, lanes), jnp.float32)
        for g in range(groups):
            spread = jnp.where(line // share == g, values(g), spread)
        return spread

    skip = per_head(2 * slabs)
    for row in range(slabs):
        gate = flat[pl.ds(row, count, stride=lines), :]
        vectors = []
        for kind in range(2):
            vector = jnp.zeros((groups, lanes), jnp.float32)
            for q in range(share):
                part = flat[pl.ds(q * lines + 2 * slabs + kind, groups, stride=share * lines), :]
                shift = (q - row) * quarter % lanes
                part = pltpu.roll(part, shift, 1) if shift else part
                vector = jnp.where(lane_of // quarter == q, part, vector)
            vectors.append(vector)
        newest = jnp.concatenate(
            [flat[pl.ds(slabs + row, count, stride=lines), :]] + vectors, axis=0
        )
        fresh[row] = newest.astype(jnp.bfloat16)
        taken = newest * taps[past].astype(jnp.float32)
        for t in range(past):
            taken += window[row * past + t].astype(jnp.float32) * taps[t].astype(jnp.float32)
        taken += bias[...]
        convolved = taken / (1.0 + jnp.exp(-taken))
        head_input = convolved[:blocks]
        write = convolved[blocks : blocks + groups]
        read = convolved[blocks + groups :]
        steps = per_head(row) * head_input
        fed[row] = steps
        written[row] = write
        overlap = jnp.sum(write * read, axis=1, keepdims=True)
        direct = by_group(lambda g: overlap[g : g + 1])
        copies[row].wait()
        columns = jnp.zeros((lanes, lanes), jnp.float32)
        for j in range(blocks):
            block = state[row, pair * j : pair * (j + 1)].reshape(lanes, lanes)
            g = j // share
            total = jnp.sum(block * read[g : g + 1], axis=1, keepdims=True)
            columns = jnp.where(wide_lane == j, total, columns)
        mixed = per_head(slabs + row) * columns.T[:blocks] + steps * direct + skip * head_input
        mixed = mixed.astype(jnp.bfloat16).astype(jnp.float32)
        gated = mixed * (gate / (1.0 + jnp.exp(-gate)))
        square = jnp.sum(gated * gated, axis=1, keepdims=True)
        total = by_group(
            lambda g: jnp.sum(square[g * share : (g + 1) * share], axis=0, keepdims=True)
        )
        scale = lax.rsqrt(total / (share * lanes) + epsilon)
        result = (gated * scale * gain[...]).astype(jnp.bfloat16)
        for z in range(far):
            out[z, row * blocks : (row + 1) * blocks] = result


def output_kernel(gathered, columns, weights_hbm, out, flat, wide, rows, weights, sems):
    copy = pltpu.make_async_copy(weights_hbm, weights, sems.at[0])
    copy.start()
    near, far, chunk, lanes = gathered.shape
    count = near * far
    blocks = weights.shape[1] // lanes
    slabs = chunk // blocks
    flat[...] = gathered[...].reshape(count * chunk, lanes).astype(jnp.float32)
    rows[slabs * count :, :] = jnp.zeros((lanes - slabs * count, blocks * lanes), jnp.bfloat16)
    for k in range(blocks):
        for row in range(slabs):
            for n in range(near):
                wide[k, pl.ds(row * count + n, far, stride=near), :] = flat[
                    pl.ds(n * far * chunk + row * blocks + k, far, stride=chunk), :
                ]
        rows[: slabs * count, k * lanes : (k + 1) * lanes] = wide[k].astype(jnp.bfloat16)
    copy.wait()
    mine = (columns[...] + contract(weights[...], rows[...], 1, 1)).astype(jnp.bfloat16)
    for z in range(out.shape[0]):
        out[z] = mine


def expert_kernel(
    place,
    gain,
    resid,
    chosen,
    gate_hbm,
    up_hbm,
    down_hbm,
    part_hbm,
    out,
    own,
    wide,
    routed,
    shared,
    staged,
    spread,
    gate,
    up,
    down,
    sems,
    part_sems,
):
    near, far, features, lanes = resid.shape
    width = near * far * features
    count = chosen.shape[0]
    slabs = own.shape[0]
    lines = out.shape[1]
    copies = [
        pltpu.make_async_copy(gate_hbm, gate, sems.at[0]),
        pltpu.make_async_copy(up_hbm, up, sems.at[1]),
        pltpu.make_async_copy(down_hbm, down, sems.at[2]),
    ]
    for copy in copies:
        copy.start()
    square = jnp.zeros((lanes, 1), jnp.float32)
    for z in range(far):
        for pair in range(near // 2):
            block = jnp.concatenate([resid[2 * pair, z], resid[2 * pair + 1, z]], axis=0)
            rows = block.astype(jnp.float32).T
            start = (z * near + 2 * pair) * features
            wide[:, start : start + 2 * features] = rows
            square += jnp.sum(rows * rows, axis=1, keepdims=True)
    me = place[0]
    first = part_hbm.shape[1] - CAP * near * features
    for n in range(near):
        for s in range(CAP):
            start = pl.multiple_of(first + (s * near + lax.rem(me, near)) * features, features)
            copies.append(
                pltpu.make_async_copy(
                    part_hbm.at[n, pl.ds(start, features)],
                    spread.at[pl.ds(n * features, features), pl.ds(s * LANES, LANES)],
                    part_sems.at[n * CAP + s],
                )
            )
    for copy in copies[3:]:
        copy.start()
    scale = lax.rsqrt(square / width + epsilon)
    values = wide[...]
    routed[...] = (values * scale * gain[...]).astype(jnp.bfloat16)
    shared[...] = (values * gain[...]).astype(jnp.bfloat16)

    for row in range(slabs):
        own[row : row + 1, :] = wide[pl.ds(row * count + me, 1), :]
    block = near * features
    for copy in copies[3:]:
        copy.wait()
    start = pl.multiple_of((me // near) * block, block)
    partial = jnp.dot(
        shared[:, pl.ds(start, block)], spread[...], preferred_element_type=jnp.float32
    )
    chunks = width // LANES
    for s in range(CAP):
        for row in range(slabs):
            staged[pl.ds(CAP * chunks + s * slabs + row, count, stride=lines), :] = partial[
                row * count : (row + 1) * count, s * LANES : (s + 1) * LANES
            ]

    copies[0].wait()
    gate_pre = jnp.dot(routed[...], gate[0], preferred_element_type=jnp.float32)
    copies[1].wait()
    up_pre = jnp.dot(routed[...], up[0], preferred_element_type=jnp.float32)
    expert_hidden = (gate_pre / (1.0 + jnp.exp(-gate_pre)) * up_pre).astype(jnp.bfloat16)

    lane = lax.broadcasted_iota(jnp.int32, (count, lanes), 1)
    line = lax.broadcasted_iota(jnp.int32, (count, lanes), 0)
    flags = chosen[:, slabs * (LANES // (slabs + 1)) :]
    picks = []
    for s in range(CAP):
        pick = jnp.zeros((count, lanes), jnp.float32)
        earlier = jnp.zeros((count, 1), jnp.float32)
        for row in range(slabs):
            flag = flags[:, row : row + 1]
            taken = jnp.where(earlier == float(s), flag, 0.0)
            pick = jnp.where(lane == row * count + line, taken, pick)
            earlier = earlier + flag
        picks.append(pick)
    pick = jnp.concatenate(picks, axis=0).astype(jnp.bfloat16)
    rows = jnp.dot(pick, expert_hidden, preferred_element_type=jnp.float32).astype(jnp.bfloat16)
    copies[2].wait()
    result = jnp.dot(rows, down[0], preferred_element_type=jnp.float32)
    for s in range(CAP):
        for k in range(chunks):
            staged[pl.ds(s * chunks + k, count, stride=lines), :] = result[
                s * count : (s + 1) * count, k * LANES : (k + 1) * LANES
            ]
    used = CAP * (chunks + slabs)
    for k in range(used, lines):
        staged[pl.ds(k, count, stride=lines), :] = jnp.zeros((count, LANES), jnp.float32)
    out[...] = staged[...].astype(jnp.bfloat16).reshape(count, lines, LANES)


def shards(
    hidden,
    conv_window,
    ssm_state,
    gate_proj,
    input_proj,
    write_proj,
    read_proj,
    step_proj,
    step_bias,
    decay_log,
    decay_shift,
    skip_scale,
    conv_taps,
    conv_bias,
    mix_gain,
    group_gain,
    out_proj,
    ffn_gain,
    router,
    expert_ids,
    expert_gate,
    expert_up,
    expert_down,
    shared_gate,
    shared_up,
    shared_down,
):
    rows = hidden.shape[0]
    width = hidden.shape[1]
    index = lax.axis_index(EP)
    count = lax.axis_size(EP)
    near = lax.axis_size(NEAR)
    experts = router.shape[1]
    units = shared_gate.shape[1]
    features = shared_gate.shape[0]

    far = lax.axis_size("zh")
    chunks = width // LANES
    place = index.astype(jnp.int32).reshape(1)
    (opening,) = fast_call(
        open_kernel,
        "open_rows",
        [((far, rows * chunks, LANES), jnp.bfloat16)],
        [((rows * chunks, LANES), jnp.float32)],
        [],
        [hidden],
        [],
    )
    opened = lax.all_to_all(opening, "zh", 0, 0, tiled=True).reshape(-1, LANES)
    later = (shared_gate, shared_up, conv_window, conv_taps, conv_bias, group_gain)
    later, _ = lax.optimization_barrier((later, opening))
    blocks = [
        jnp.moveaxis(weights.reshape(features, near, LANES), 1, 0).reshape(-1, LANES)
        for weights in later[:2]
    ]
    span = conv_bias.shape[0] // LANES
    window_blocks = later[2].reshape(-1, span, LANES)
    taps_blocks = later[3].reshape(-1, span, LANES)
    bias_blocks = later[4].reshape(-1, LANES)
    group_gain = later[5].reshape(-1, LANES)
    gathered = lax.all_gather(jnp.concatenate([opened, *blocks], axis=0), NEAR)
    col_width = out_proj.shape[1]
    message, resid_cols = fast_call(
        project_kernel,
        "project_rows",
        [((count, 8, LANES), jnp.bfloat16), ((col_width, LANES), jnp.float32)],
        [
            ((count * rows * chunks, LANES), jnp.float32),
            ((chunks, count * rows, LANES), jnp.float32),
            ((count * rows, width), jnp.bfloat16),
            ((count * 8, LANES), jnp.float32),
        ],
        [place, expert_ids],
        [mix_gain.reshape(1, width)],
        [gathered],
        [gate_proj, input_proj, write_proj.T, read_proj.T],
    )
    pieces = lax.all_to_all(message, EP, 0, 0, tiled=True)

    later = (hidden, decay_shift, step_bias, decay_log, skip_scale)
    later, _ = lax.optimization_barrier((later, message))
    hidden_later, decay_shift, step_bias, decay_log, skip_scale = later
    hidden_wide = hidden_later.astype(jnp.float32)
    normed_local = (hidden_wide * row_scale(hidden_wide) * mix_gain).astype(jnp.bfloat16)
    step_raw = matmul(normed_local, step_proj)

    inner_width = out_proj.shape[0]
    blocks = inner_width // LANES
    step_size = jax.nn.softplus(step_raw + step_bias)
    decay_rate = jnp.exp(decay_shift - step_size * jnp.exp(decay_log))
    heads = jnp.concatenate([step_size, decay_rate, skip_scale[None]], axis=0)
    heads = jnp.pad(heads, ((0, LANES - heads.shape[0]), (0, 0))).T
    gated_rows, fresh, fed, write_vec, chosen = fast_call(
        mixer_kernel,
        "mix_rows",
        [
            ((far, rows * blocks, LANES), jnp.bfloat16),
            ((rows, span, LANES), jnp.bfloat16),
            ((rows, blocks, LANES), jnp.float32),
            ((rows, GROUPS, STATE), jnp.float32),
            ((count, LANES), jnp.float32),
        ],
        [((count * 8, LANES), jnp.float32)],
        [],
        [group_gain, bias_blocks],
        [heads, window_blocks, taps_blocks, pieces],
        [ssm_state],
    )
    gated_all = near_gather(gated_rows)
    (resid_part,) = fast_call(
        output_kernel,
        "output_rows",
        [((far, col_width, LANES), jnp.bfloat16)],
        [
            ((count * rows * inner_width // LANES, LANES), jnp.float32),
            ((inner_width // LANES, rows * count, LANES), jnp.float32),
            ((LANES, inner_width), jnp.bfloat16),
        ],
        [],
        [],
        [gated_all, resid_cols],
        [out_proj.T],
    )
    resid_all = near_gather(resid_part)
    used = CAP * (chunks + rows)
    outbound, resid_own = fast_call(
        expert_kernel,
        "expert_rows",
        [((count, -(-used // 8) * 8, LANES), jnp.bfloat16), ((rows, width), jnp.float32)],
        [
            ((LANES, width), jnp.float32),
            ((LANES, width), jnp.bfloat16),
            ((LANES, width), jnp.bfloat16),
            ((count * -(-used // 8) * 8, LANES), jnp.float32),
            ((near * features, CAP * LANES), jnp.bfloat16),
        ],
        [place],
        [ffn_gain.reshape(1, width)],
        [resid_all, chosen],
        [expert_gate, expert_up, expert_down],
        [gathered],
    )
    returned = lax.all_to_all(outbound, EP, 0, 0, tiled=True)

    later = (expert_ids, conv_window, fresh, fed, write_vec, decay_rate)
    later, _ = lax.optimization_barrier((later, outbound))
    expert_ids, conv_window, fresh, fed, write_vec, decay_rate = later
    next_window = jnp.concatenate([conv_window[:, 1:], fresh.reshape(rows, 1, -1)], axis=1)
    per_group = step_size.shape[1] // GROUPS
    next_state = (
        decay_rate[:, :, None, None] * ssm_state
        + fed.reshape(rows, -1, HEAD_DIM)[..., None]
        * jnp.repeat(write_vec, per_group, axis=1)[:, :, None, :]
    )
    member = jnp.any(
        expert_ids[:, :, None] == jnp.arange(experts, dtype=jnp.int32)[None, None, :], axis=1
    )
    norm_scale = row_scale(resid_own)
    routed_own = (resid_own * norm_scale * ffn_gain).astype(jnp.bfloat16)
    scores = jnp.where(member, jax.nn.sigmoid(matmul(routed_own, router)), 0.0)
    weights = routed_scale * scores / jnp.sum(scores, axis=1, keepdims=True)
    own_member = member.astype(jnp.int32)
    own_slot = jnp.cumsum(own_member, axis=0) - own_member
    by_slot = jnp.concatenate([jnp.where(own_slot == s, weights, 0.0) for s in range(CAP)], axis=1)
    back = returned[:, : CAP * chunks].reshape(count, CAP, width)
    back = jnp.moveaxis(back, 1, 0).reshape(CAP * count, width)
    high, low = split_pair(by_slot)
    routed = matmul(high, back) + matmul(low, back)
    pre = returned[:, CAP * chunks : used].reshape(far, near, 2, rows, units // near)
    pre = jnp.sum(pre.astype(jnp.float32), axis=0).transpose(1, 2, 0, 3).reshape(2, rows, units)
    shared_hidden = (jax.nn.silu(norm_scale * pre[0]) * (norm_scale * pre[1])).astype(jnp.bfloat16)
    layer_out = (resid_own + routed + matmul(shared_hidden, shared_down)).astype(jnp.bfloat16)
    return (layer_out, next_state, next_window)


def solution(mesh):
    torus = Mesh(mesh.devices.reshape(mesh.shape["grp"], -1, 2, 2), GRP_EP)
    return jax.shard_map(
        shards,
        mesh=torus,
        in_specs=(
            P(GRP_EP, None),
            P(GRP_EP, None, None),
            P(GRP_EP, None, None, None),
            P(None, EP),
            P(None, EP),
            P(None, EP),
            P(None, EP),
            P(),
            P(),
            P(),
            P(GRP_EP, None),
            P(),
            P(),
            P(),
            P(),
            P(),
            P(None, EP),
            P(),
            P(),
            P(GRP_EP, None),
            P(EP, None, None),
            P(EP, None, None),
            P(EP, None, None),
            P(EP, None),
            P(EP, None),
            P(),
        ),
        out_specs=(P(GRP_EP, None), P(GRP_EP, None, None, None), P(GRP_EP, None, None)),
        check_vma=False,
    )
```

```python
import jax
import jax.numpy as jnp
from jax import lax
from jax.sharding import Mesh
from jax.experimental import pallas as pl
from jax.experimental.pallas import tpu as pltpu
from jax.sharding import PartitionSpec as P

HEAD_DIM = 64
GROUPS = 8
STATE = 128
CAP = 2
EP = ("zh", "zl", "core")
NEAR = ("zl", "core")
GRP_EP = ("grp",) + EP
LANES = 128

epsilon = 1e-06
routed_scale = 2.5


def row_scale(values):
    return lax.rsqrt(jnp.mean(values * values, axis=-1, keepdims=True) + epsilon)


def matmul(left, right):
    return jnp.dot(left, right, preferred_element_type=jnp.float32)


def contract(left, right, left_dim, right_dim):
    return lax.dot_general(
        left, right, (((left_dim,), (right_dim,)), ((), ())), preferred_element_type=jnp.float32
    )


def split_pair(values):
    high = values.astype(jnp.bfloat16)
    low = (values - high.astype(jnp.float32)).astype(jnp.bfloat16)
    return high, low


def near_gather(copies):
    return lax.all_gather(lax.all_to_all(copies, "zh", 0, 0, tiled=True), NEAR)


def kept_in(space, arrays):
    return [pltpu.with_memory_space_constraint(array, space) for array in arrays]


class Late:
    def __init__(self, source, landing, sem):
        self.copy = pltpu.make_async_copy(source, landing, sem)
        self.landing = landing
        self.shape = landing.shape
        self.here = False

    def __getitem__(self, place):
        if not self.here:
            self.copy.wait()
            self.here = True
        return self.landing[place]


def fast_call(kernel, outs, scratch, scalars, fetched, arrays, far=[], remote=[]):
    vmem = pl.BlockSpec(memory_space=pltpu.VMEM)
    hbm = pl.BlockSpec(memory_space=pltpu.HBM)
    late = len(scalars) + len(fetched)
    specs = [hbm] * late + [vmem] * len(arrays) + [hbm] * (len(far) + len(remote))
    landing = [pltpu.VMEM(array.shape, array.dtype) for array in far]
    waits = [pltpu.SemaphoreType.DMA((4,))] if far else []
    waits += [pltpu.SemaphoreType.DMA((8,))] if remote else []
    ends = [pltpu.SMEM(array.shape, array.dtype) for array in scalars]
    ends += [pltpu.VMEM(array.shape, array.dtype) for array in fetched]
    ends += [pltpu.SemaphoreType.DMA((late,))] if late else []

    def body(*refs):
        if not late:
            return kernel(*refs)
        sems = refs[-1]
        operands = [
            Late(refs[k], refs[len(refs) - 1 - late + k], sems.at[k]) for k in range(late)
        ]
        for operand in operands:
            operand.copy.start()
        kernel(*operands, *refs[late : len(refs) - 1 - late])
        assert all(operand.here for operand in operands)

    return pl.pallas_call(
        body,
        out_shape=tuple(pltpu.VMEM(shape, dtype) for shape, dtype in outs),
        in_specs=specs,
        out_specs=(vmem,) * len(outs),
        scratch_shapes=[pltpu.VMEM(shape, dtype) for shape, dtype in scratch]
        + landing
        + waits
        + ends,
        compiler_params=pltpu.CompilerParams(vmem_limit_bytes=24 * 1024 * 1024),
    )(
        *kept_in(pltpu.HBM, scalars + fetched),
        *kept_in(pltpu.VMEM, arrays),
        *kept_in(pltpu.HBM, far + remote),
    )


def open_kernel(hidden, out, staged):
    rows, width = hidden.shape
    chunks = width // LANES
    values = hidden[...].astype(jnp.float32)
    for k in range(chunks):
        staged[pl.ds(k, rows, stride=chunks), :] = values[:, k * LANES : (k + 1) * LANES]
    mine = staged[...].astype(jnp.bfloat16)
    for z in range(out.shape[0]):
        out[z] = mine


def project_kernel(
    place,
    ids,
    gain,
    gathered,
    gate_hbm,
    input_hbm,
    write_hbm,
    read_hbm,
    message,
    columns,
    flat,
    wide,
    normed,
    staged,
    gate_weights,
    input_weights,
    write_weights,
    read_weights,
    sems,
):
    copies = [
        pltpu.make_async_copy(gate_hbm, gate_weights, sems.at[0]),
        pltpu.make_async_copy(input_hbm, input_weights, sems.at[1]),
        pltpu.make_async_copy(write_hbm, write_weights, sems.at[2]),
        pltpu.make_async_copy(read_hbm, read_weights, sems.at[3]),
    ]
    for copy in copies:
        copy.start()
    near, _, lanes = gathered.shape
    count, lines, _ = message.shape
    far = count // near
    rows = ids.shape[0]
    blocks = gain.shape[1] // lanes
    chunk = rows * blocks
    flat[...] = (
        gathered[:, : far * chunk, :].reshape(count * chunk, lanes).astype(jnp.float32)
    )
    square = jnp.zeros((rows * count, 1), jnp.float32)
    for k in range(blocks):
        for row in range(rows):
            for n in range(near):
                wide[k, pl.ds(row * count + n, far, stride=near), :] = flat[
                    pl.ds(n * far * chunk + row * blocks + k, far, stride=chunk), :
                ]
        part = wide[k]
        square += jnp.sum(part * part, axis=1, keepdims=True)
    scale = lax.rsqrt(square / (blocks * lanes) + epsilon)
    for k in range(blocks):
        span = slice(k * lanes, (k + 1) * lanes)
        normed[:, span] = (wide[k] * scale * gain[:, span]).astype(jnp.bfloat16)
    values = normed[...]
    for copy in copies:
        copy.wait()
    gate_part = jnp.dot(values, gate_weights[...], preferred_element_type=jnp.float32)
    input_part = jnp.dot(values, input_weights[...], preferred_element_type=jnp.float32)
    write_part = contract(values, write_weights[...], 1, 1)
    read_part = contract(values, read_weights[...], 1, 1)

    def of_row(part, row):
        return part[row * count : (row + 1) * count]

    small = lanes - rows * write_part.shape[1]
    expert = lax.broadcasted_iota(jnp.int32, (count, small), 0)
    lane = lax.broadcasted_iota(jnp.int32, (count, small), 1)
    member = jnp.zeros((count, small), jnp.float32)
    for row in range(rows):
        for k in range(ids.shape[1]):
            member = jnp.where((lane == row) & (expert == ids[row, k]), 1.0, member)
    for row in range(rows):
        staged[pl.ds(row, count, stride=lines), :] = of_row(gate_part, row)
        staged[pl.ds(rows + row, count, stride=lines), :] = of_row(input_part, row)
    staged[pl.ds(2 * rows, count, stride=lines), :] = jnp.concatenate(
        [of_row(write_part, row) for row in range(rows)] + [member], axis=1
    )
    staged[pl.ds(2 * rows + 1, count, stride=lines), :] = jnp.concatenate(
        [of_row(read_part, row) for row in range(rows)] + [jnp.zeros_like(member)], axis=1
    )
    message[...] = staged[...].astype(jnp.bfloat16).reshape(count, lines, lanes)

    me = place[0]
    for half in range(2):
        for row in range(rows):
            columns[row * far : (row + 1) * far, half * lanes : (half + 1) * lanes] = wide[
                2 * (me // near) + half,
                pl.ds(row * count + lax.rem(me, near), far, stride=near),
                :,
            ]


def mixer_kernel(
    gain, bias, heads, window, taps, pieces, state_hbm, out, fresh, fed, written, named, flat, state, sems
):
    far = out.shape[0]
    slabs = fresh.shape[0]
    past = taps.shape[0] - 1
    count, lines, lanes = pieces.shape
    groups = written.shape[1]
    blocks = fed.shape[1]
    share = blocks // groups
    quarter = lanes // share
    pair = lanes // state.shape[2]
    copies = [
        pltpu.make_async_copy(state_hbm.at[row], state.at[row], sems.at[row])
        for row in range(slabs)
    ]
    for copy in copies:
        copy.start()
    flat[...] = pieces[...].reshape(count * lines, lanes).astype(jnp.float32)
    named[...] = flat[pl.ds(2 * slabs, count, stride=lines), :]
    line = lax.broadcasted_iota(jnp.int32, (blocks, lanes), 0)
    lane = lax.broadcasted_iota(jnp.int32, (blocks, lanes), 1)
    lane_of = lax.broadcasted_iota(jnp.int32, (groups, lanes), 1)
    wide_lane = lax.broadcasted_iota(jnp.int32, (lanes, lanes), 1)
    even = heads[pl.ds(0, blocks, stride=pair), :]
    odd = heads[pl.ds(1, blocks, stride=pair), :]

    def per_head(column):
        return jnp.where(
            lane < lanes // 2, even[:, column : column + 1], odd[:, column : column + 1]
        )

    def by_group(values):
        spread = jnp.zeros((blocks, lanes), jnp.float32)
        for g in range(groups):
            spread = jnp.where(line // share == g, values(g), spread)
        return spread

    skip = per_head(2 * slabs)
    for row in range(slabs):
        gate = flat[pl.ds(row, count, stride=lines), :]
        vectors = []
        for kind in range(2):
            vector = jnp.zeros((groups, lanes), jnp.float32)
            for q in range(share):
                part = flat[pl.ds(q * lines + 2 * slabs + kind, groups, stride=share * lines), :]
                shift = (q - row) * quarter % lanes
                part = pltpu.roll(part, shift, 1) if shift else part
                vector = jnp.where(lane_of // quarter == q, part, vector)
            vectors.append(vector)
        newest = jnp.concatenate(
            [flat[pl.ds(slabs + row, count, stride=lines), :]] + vectors, axis=0
        )
        fresh[row] = newest.astype(jnp.bfloat16)
        taken = newest * taps[past].astype(jnp.float32)
        for t in range(past):
            taken += window[row * past + t].astype(jnp.float32) * taps[t].astype(jnp.float32)
        taken += bias[...]
        convolved = taken / (1.0 + jnp.exp(-taken))
        head_input = convolved[:blocks]
        write = convolved[blocks : blocks + groups]
        read = convolved[blocks + groups :]
        steps = per_head(row) * head_input
        fed[row] = steps
        written[row] = write
        overlap = jnp.sum(write * read, axis=1, keepdims=True)
        direct = by_group(lambda g: overlap[g : g + 1])
        copies[row].wait()
        columns = jnp.zeros((lanes, lanes), jnp.float32)
        for j in range(blocks):
            block = state[row, pair * j : pair * (j + 1)].reshape(lanes, lanes)
            g = j // share
            total = jnp.sum(block * read[g : g + 1], axis=1, keepdims=True)
            columns = jnp.where(wide_lane == j, total, columns)
        mixed = per_head(slabs + row) * columns.T[:blocks] + steps * direct + skip * head_input
        mixed = mixed.astype(jnp.bfloat16).astype(jnp.float32)
        gated = mixed * (gate / (1.0 + jnp.exp(-gate)))
        square = jnp.sum(gated * gated, axis=1, keepdims=True)
        total = by_group(
            lambda g: jnp.sum(square[g * share : (g + 1) * share], axis=0, keepdims=True)
        )
        scale = lax.rsqrt(total / (share * lanes) + epsilon)
        result = (gated * scale * gain[...]).astype(jnp.bfloat16)
        for z in range(far):
            out[z, row * blocks : (row + 1) * blocks] = result


def output_kernel(
    place, across, columns, mine_hbm, *refs
):
    others, (out, flat, rows, weights, sems) = refs[:-5], refs[-5:]
    near = 1 + len(others)
    me = lax.rem(place[0], near)
    features = mine_hbm.shape[0]
    copies = []
    for x, source in enumerate((mine_hbm, *others)):
        start = pl.multiple_of(lax.bitwise_xor(me, x) * features, features)
        copies.append(
            pltpu.make_async_copy(source, weights.at[pl.ds(start, features)], sems.at[x])
        )
    for copy in copies:
        copy.start()
    far, chunk, lanes = across.shape
    blocks = weights.shape[1] // lanes
    slabs = chunk // blocks
    flat[...] = across[...].reshape(far * chunk, lanes).astype(jnp.float32)
    for k in range(blocks):
        part = jnp.concatenate(
            [flat[pl.ds(row * blocks + k, far, stride=chunk), :] for row in range(slabs)], axis=0
        )
        rows[:, k * lanes : (k + 1) * lanes] = part.astype(jnp.bfloat16)
    for copy in copies:
        copy.wait()
    mine = columns[...] + contract(rows[...], weights[...], 1, 1)
    lines = jnp.concatenate([mine[:, :lanes], mine[:, lanes:]], axis=0).astype(jnp.bfloat16)
    for z in range(out.shape[0]):
        out[z] = lines


def expert_kernel(
    place,
    gain,
    resid,
    chosen,
    gate_hbm,
    up_hbm,
    down_hbm,
    part_hbm,
    out,
    own,
    wide,
    routed,
    shared,
    staged,
    spread,
    gate,
    up,
    down,
    sems,
    part_sems,
):
    near, far, _, lanes = resid.shape
    slabs, width = own.shape
    features = width // (near * far)
    count = near * far
    seqs = slabs * far
    lines = out.shape[1]
    copies = [
        pltpu.make_async_copy(gate_hbm, gate, sems.at[0]),
        pltpu.make_async_copy(up_hbm, up, sems.at[1]),
        pltpu.make_async_copy(down_hbm, down, sems.at[2]),
    ]
    for copy in copies:
        copy.start()
    wide[near * seqs :, :] = jnp.zeros((lanes - near * seqs, width), jnp.float32)
    for n in range(near):
        for z in range(far):
            block = resid[n, z].astype(jnp.float32)
            for half in range(2):
                start = (2 * z + half) * lanes
                wide[n * seqs : (n + 1) * seqs, start : start + lanes] = block[
                    half * seqs : (half + 1) * seqs
                ]
    square = jnp.sum(wide[...] * wide[...], axis=1, keepdims=True)
    me = place[0]
    first = part_hbm.shape[1] - CAP * near * features
    for n in range(near):
        for s in range(CAP):
            start = pl.multiple_of(first + (s * near + lax.rem(me, near)) * features, features)
            copies.append(
                pltpu.make_async_copy(
                    part_hbm.at[n, pl.ds(start, features)],
                    spread.at[pl.ds(n * features, features), pl.ds(s * LANES, LANES)],
                    part_sems.at[n * CAP + s],
                )
            )
    for copy in copies[3:]:
        copy.start()
    scale = lax.rsqrt(square / width + epsilon)
    values = wide[...]
    routed[...] = (values * scale * gain[...]).astype(jnp.bfloat16)
    shared[...] = (values * gain[...]).astype(jnp.bfloat16)

    for row in range(slabs):
        mine = lax.rem(me, near) * seqs + row * far + me // near
        own[row : row + 1, :] = wide[pl.ds(mine, 1), :]
    block = near * features
    for copy in copies[3:]:
        copy.wait()
    start = pl.multiple_of((me // near) * block, block)
    partial = jnp.dot(
        shared[:, pl.ds(start, block)], spread[...], preferred_element_type=jnp.float32
    )
    chunks = width // LANES
    for s in range(CAP):
        for row in range(slabs):
            for n in range(near):
                first = n * seqs + row * far
                staged[
                    pl.ds(n * lines + CAP * chunks + s * slabs + row, far, stride=near * lines), :
                ] = partial[first : first + far, s * LANES : (s + 1) * LANES]

    copies[0].wait()
    gate_pre = jnp.dot(routed[...], gate[0], preferred_element_type=jnp.float32)
    copies[1].wait()
    up_pre = jnp.dot(routed[...], up[0], preferred_element_type=jnp.float32)
    expert_hidden = (gate_pre / (1.0 + jnp.exp(-gate_pre)) * up_pre).astype(jnp.bfloat16)

    lane = lax.broadcasted_iota(jnp.int32, (count, lanes), 1)
    line = lax.broadcasted_iota(jnp.int32, (count, lanes), 0)
    flags = chosen[:, slabs * (LANES // (slabs + 1)) :]
    picks = []
    for s in range(CAP):
        pick = jnp.zeros((count, lanes), jnp.float32)
        earlier = jnp.zeros((count, 1), jnp.float32)
        for row in range(slabs):
            flag = flags[:, row : row + 1]
            taken = jnp.where(earlier == float(s), flag, 0.0)
            spot = lax.rem(line, near) * seqs + row * far + line // near
            pick = jnp.where(lane == spot, taken, pick)
            earlier = earlier + flag
        picks.append(pick)
    pick = jnp.concatenate(picks, axis=0).astype(jnp.bfloat16)
    rows = jnp.dot(pick, expert_hidden, preferred_element_type=jnp.float32).astype(jnp.bfloat16)
    copies[2].wait()
    result = jnp.dot(rows, down[0], preferred_element_type=jnp.float32)
    for s in range(CAP):
        for k in range(chunks):
            staged[pl.ds(s * chunks + k, count, stride=lines), :] = result[
                s * count : (s + 1) * count, k * LANES : (k + 1) * LANES
            ]
    used = CAP * (chunks + slabs)
    for k in range(used, lines):
        staged[pl.ds(k, count, stride=lines), :] = jnp.zeros((count, LANES), jnp.float32)
    out[...] = staged[...].astype(jnp.bfloat16).reshape(count, lines, LANES)


def shards(
    hidden,
    conv_window,
    ssm_state,
    gate_proj,
    input_proj,
    write_proj,
    read_proj,
    step_proj,
    step_bias,
    decay_log,
    decay_shift,
    skip_scale,
    conv_taps,
    conv_bias,
    mix_gain,
    group_gain,
    out_proj,
    ffn_gain,
    router,
    expert_ids,
    expert_gate,
    expert_up,
    expert_down,
    shared_gate,
    shared_up,
    shared_down,
):
    rows = hidden.shape[0]
    width = hidden.shape[1]
    index = lax.axis_index(EP)
    count = lax.axis_size(EP)
    near = lax.axis_size(NEAR)
    experts = router.shape[1]
    units = shared_gate.shape[1]
    features = shared_gate.shape[0]

    far = lax.axis_size("zh")
    col_width = out_proj.shape[1]
    chunks = width // LANES
    place = index.astype(jnp.int32).reshape(1)
    (opening,) = fast_call(
        open_kernel,
        [((far, rows * chunks, LANES), jnp.bfloat16)],
        [((rows * chunks, LANES), jnp.float32)],
        [],
        [hidden],
        [],
    )
    opened = lax.all_to_all(opening, "zh", 0, 0, tiled=True).reshape(-1, LANES)
    later = (shared_gate, shared_up, conv_window, conv_taps, conv_bias, group_gain)
    later, _ = lax.optimization_barrier((later, opening))
    blocks = [
        jnp.moveaxis(weights.reshape(features, near, LANES), 1, 0).reshape(-1, LANES)
        for weights in later[:2]
    ]
    span = conv_bias.shape[0] // LANES
    window_blocks = later[2].reshape(-1, span, LANES)
    taps_blocks = later[3].reshape(-1, span, LANES)
    bias_blocks = later[4].reshape(-1, LANES)
    group_gain = later[5].reshape(-1, LANES)
    gathered = lax.all_gather(jnp.concatenate([opened, *blocks], axis=0), NEAR)
    message, resid_cols = fast_call(
        project_kernel,
        [((count, 8, LANES), jnp.bfloat16), ((rows * far, near * col_width), jnp.float32)],
        [
            ((count * rows * chunks, LANES), jnp.float32),
            ((chunks, count * rows, LANES), jnp.float32),
            ((count * rows, width), jnp.bfloat16),
            ((count * 8, LANES), jnp.float32),
        ],
        [place, expert_ids],
        [mix_gain.reshape(1, width)],
        [gathered],
        [gate_proj, input_proj, write_proj.T, read_proj.T],
    )
    pieces = lax.all_to_all(message, EP, 0, 0, tiled=True)

    own_proj, _ = lax.optimization_barrier((out_proj.T, message))
    other_projs = [
        lax.ppermute(own_proj, NEAR, [(k, k ^ x) for k in range(near)])
        for x in range(1, near)
    ]

    later = (hidden, decay_shift, step_bias, decay_log, skip_scale)
    later, _ = lax.optimization_barrier((later, message))
    hidden_later, decay_shift, step_bias, decay_log, skip_scale = later
    hidden_wide = hidden_later.astype(jnp.float32)
    normed_local = (hidden_wide * row_scale(hidden_wide) * mix_gain).astype(jnp.bfloat16)
    step_raw = matmul(normed_local, step_proj)

    inner_width = out_proj.shape[0]
    blocks = inner_width // LANES
    step_size = jax.nn.softplus(step_raw + step_bias)
    decay_rate = jnp.exp(decay_shift - step_size * jnp.exp(decay_log))
    heads = jnp.concatenate([step_size, decay_rate, skip_scale[None]], axis=0)
    heads = jnp.pad(heads, ((0, LANES - heads.shape[0]), (0, 0))).T
    gated_rows, fresh, fed, write_vec, chosen = fast_call(
        mixer_kernel,
        [
            ((far, rows * blocks, LANES), jnp.bfloat16),
            ((rows, span, LANES), jnp.bfloat16),
            ((rows, blocks, LANES), jnp.float32),
            ((rows, GROUPS, STATE), jnp.float32),
            ((count, LANES), jnp.float32),
        ],
        [((count * 8, LANES), jnp.float32)],
        [],
        [group_gain, bias_blocks],
        [heads, window_blocks, taps_blocks, pieces],
        [ssm_state],
    )

    across = lax.all_to_all(gated_rows, "zh", 0, 0, tiled=True)
    (resid_part,) = fast_call(
        output_kernel,
        [((far, 2 * rows * far, LANES), jnp.bfloat16)],
        [
            ((count // near * rows * blocks, LANES), jnp.float32),
            ((rows * far, inner_width), jnp.bfloat16),
            ((near * col_width, inner_width), jnp.bfloat16),
        ],
        [place],
        [],
        [across, resid_cols],
        [],
        [out_proj.T, *other_projs],
    )
    resid_all = near_gather(resid_part)
    used = CAP * (chunks + rows)
    outbound, resid_own = fast_call(
        expert_kernel,
        [((count, -(-used // 8) * 8, LANES), jnp.bfloat16), ((rows, width), jnp.float32)],
        [
            ((LANES, width), jnp.float32),
            ((LANES, width), jnp.bfloat16),
            ((LANES, width), jnp.bfloat16),
            ((count * -(-used // 8) * 8, LANES), jnp.float32),
            ((near * features, CAP * LANES), jnp.bfloat16),
        ],
        [place],
        [ffn_gain.reshape(1, width)],
        [resid_all, chosen],
        [expert_gate, expert_up, expert_down],
        [gathered],
    )
    returned = lax.all_to_all(outbound, EP, 0, 0, tiled=True)

    later = (expert_ids, conv_window, fresh, fed, write_vec, decay_rate)
    later, _ = lax.optimization_barrier((later, outbound))
    expert_ids, conv_window, fresh, fed, write_vec, decay_rate = later
    next_window = jnp.concatenate([conv_window[:, 1:], fresh.reshape(rows, 1, -1)], axis=1)
    per_group = step_size.shape[1] // GROUPS
    next_state = (
        decay_rate[:, :, None, None] * ssm_state
        + fed.reshape(rows, -1, HEAD_DIM)[..., None]
        * jnp.repeat(write_vec, per_group, axis=1)[:, :, None, :]
    )
    member = jnp.any(
        expert_ids[:, :, None] == jnp.arange(experts, dtype=jnp.int32)[None, None, :], axis=1
    )
    norm_scale = row_scale(resid_own)
    routed_own = (resid_own * norm_scale * ffn_gain).astype(jnp.bfloat16)
    scores = jnp.where(member, jax.nn.sigmoid(matmul(routed_own, router)), 0.0)
    weights = routed_scale * scores / jnp.sum(scores, axis=1, keepdims=True)
    own_member = member.astype(jnp.int32)
    own_slot = jnp.cumsum(own_member, axis=0) - own_member
    by_slot = jnp.concatenate([jnp.where(own_slot == s, weights, 0.0) for s in range(CAP)], axis=1)
    back = returned[:, : CAP * chunks].reshape(count, CAP, width)
    back = jnp.moveaxis(back, 1, 0).reshape(CAP * count, width)
    high, low = split_pair(by_slot)
    routed = matmul(high, back) + matmul(low, back)
    pre = returned[:, CAP * chunks : used].reshape(far, near, 2, rows, units // near)
    pre = jnp.sum(pre.astype(jnp.float32), axis=0).transpose(1, 2, 0, 3).reshape(2, rows, units)
    shared_hidden = (jax.nn.silu(norm_scale * pre[0]) * (norm_scale * pre[1])).astype(jnp.bfloat16)
    layer_out = (resid_own + routed + matmul(shared_hidden, shared_down)).astype(jnp.bfloat16)
    return (layer_out, next_state, next_window)


def solution(mesh):
    torus = Mesh(mesh.devices.reshape(mesh.shape["grp"], -1, 2, 2), GRP_EP)
    return jax.shard_map(
        shards,
        mesh=torus,
        in_specs=(
            P(GRP_EP, None),
            P(GRP_EP, None, None),
            P(GRP_EP, None, None, None),
            P(None, EP),
            P(None, EP),
            P(None, EP),
            P(None, EP),
            P(),
            P(),
            P(),
            P(GRP_EP, None),
            P(),
            P(),
            P(),
            P(),
            P(),
            P(None, EP),
            P(),
            P(),
            P(GRP_EP, None),
            P(EP, None, None),
            P(EP, None, None),
            P(EP, None, None),
            P(EP, None),
            P(EP, None),
            P(),
        ),
        out_specs=(P(GRP_EP, None), P(GRP_EP, None, None, None), P(GRP_EP, None, None)),
        check_vma=False,
    )
```
